512 devices in a mesh: tp: 512 (over z, y, x, core).
Axes of the slice: x: 4, y: 4, z: 16, core: 2. Of those that a mesh axis runs over, the one named last changes fastest.
Arguments:
- tokens: bfloat16 [4096, 256], P('tp'), may hold values from -20 to 20, as said below
- positions: int32 [256], replicated, may hold values from 1 to 3072, 262144 in all
- norm_gain: float32 [4096], replicated, may hold values from 0.1 to 1.9
- w_query: bfloat16 [1024, 4096], P('tp'), may hold values from -0.09375 to 0.09375
- w_key: bfloat16 [1024, 4096], P('tp'), may hold values from -0.09375 to 0.09375
- w_value: bfloat16 [2048, 4096], P('tp'), may hold values from -0.09375 to 0.09375
- w_outgate: bfloat16 [2048, 4096], P('tp'), may hold values from -0.09375 to 0.09375
- w_input: bfloat16 [4, 4096], replicated, may hold values from -0.09375 to 0.09375
- w_forget: bfloat16 [4, 4096], replicated, may hold values from -0.09375 to 0.09375
- bias_input: float32 [4], replicated, may hold values from -3 to 3
- bias_forget: float32 [4], replicated, may hold values from -1 to 4
- w_read: bfloat16 [4096, 2048], P('tp'), may hold values from -0.125 to 0.125
- cells: float32 [2048, 256, 256], P('tp'), may hold values from -4 to 4
- norms: float32 [1024, 256], replicated, may hold values from 0 to 0.5
- maxima: float32 [4, 256], replicated, may hold values from -1 to 1
Outputs:
- mixed_rows: bfloat16 [4096, 256], P('tp')
- new_cells: float32 [2048, 256, 256], P('tp')
- new_norms: float32 [1024, 256], replicated
- new_maxima: float32 [4, 256], replicated
The draws below stay inside these ranges and needn't reach their ends.
Inputs may be any that keep to these rules, and one draw needn't show every extreme that they name: `tokens`: feature rows have their own scales, spread over a factor of ten.
All inputs are finite; a program needn't handle non-finite values.
Results may differ from the reference program's by a relative error of at most 0.0062.
The reference program's roundings to bfloat16 on the way (of `normed`, `query`, `key` and `gated`) count: a program that leaves them out, or rounds other values in their place, can miss the bound.
Values may be sent and summed in bfloat16 or wider, within the bound.
A program may use at most 64 MiB of HBM per device.

```python
import math
import jax
import jax.numpy as jnp
import numpy as np
from jax import lax

D = 4096
HEADS = 4
DQK = 256
DV = 512
BATCH = 256
MEAN_LEN = 1024
MOST_LEN = 3072


def draw_tokens(key, part):
    first, second = jax.random.split(key)
    row_scale = jnp.exp(jax.random.uniform(second, (D, 1), jnp.float32, -1.2, 1.2))
    base = jnp.clip(jax.random.normal(first, (D, BATCH), jnp.float32), -6.0, 6.0)
    return (base * row_scale).astype(jnp.bfloat16)


def level_of(key, dims, cuts, least, largest):
    factor_of = 1.0
    for axis_at, shards_of in cuts:
        draws = jax.random.uniform(jax.random.fold_in(jax.random.fold_in(key, 6), axis_at), (shards_of,), jnp.float32, least / len(cuts), largest / len(cuts))
        factor_of = factor_of * jnp.repeat(jnp.exp(draws), dims[axis_at] // shards_of).reshape((-1,) + (1,) * (len(dims) - 1 - axis_at))
    return factor_of


def length_profile(number_of, total, reach, slope):
    loads = [(1 << 20) // math.isqrt(rank ** slope) + 1 for rank in range(2, number_of + 1)]
    rest, counts = total - reach - (number_of - 1), [1] * (number_of - 1)
    while rest > 0:
        candidates = [i for i in range(number_of - 1) if counts[i] < reach]
        whole, remaining = sum([loads[i] for i in candidates]), rest
        for i in candidates:
            addition = min(reach - counts[i], max(1, remaining * loads[i] // whole), rest)
            counts[i] = counts[i] + addition
            rest = rest - addition
    return np.array([reach] + counts)


def ragged(stream_key, count, total, limit, lean):
    if count == 2:
        one = jax.random.randint(stream_key, (), max(1, total - limit), min(limit, total - 1) + 1)
        return jnp.stack([one, total - one])
    tallies = jnp.asarray(length_profile(count, total, limit, lean), jnp.int32)
    couples = (count - 1) // 2
    donor, taker = tallies[1:1 + 2 * couples:2], tallies[2:2 + 2 * couples:2]
    margin = jnp.minimum(donor - 1, limit - taker)
    moved = jax.random.randint(jax.random.fold_in(stream_key, 1), (couples,), 0, 1 << 20) % (margin + 1)
    tallies = tallies.at[1:1 + 2 * couples:2].set(donor - moved).at[2:2 + 2 * couples:2].set(taker + moved)
    return tallies[jax.random.permutation(jax.random.fold_in(stream_key, 2), count)]


def bell_draw(stream_key, dims, scale, most, cuts=(), kind=jnp.bfloat16):
    level = level_of(stream_key, dims, cuts, -0.22, 0.18) if cuts else 1.0
    drawn = jax.random.normal(stream_key, dims, jnp.float32) * scale * level
    return jnp.minimum(jnp.maximum(drawn, -most), most).astype(kind)


def setup_inputs(seed: int = 0) -> dict:
    arg_keys = jax.random.split(jax.random.key(seed), 16)
    tokens = draw_tokens(jax.random.fold_in(arg_keys[15], 71), 0)
    positions = ragged(arg_keys[1], BATCH, BATCH * MEAN_LEN, MOST_LEN, 2).astype(jnp.int32)
    norm_gain = jnp.clip(1.0 + 0.18 * jax.random.normal(arg_keys[2], (D,), jnp.float32), 0.1, 1.9)
    w_query = bell_draw(arg_keys[3], (HEADS * DQK, D), D ** -0.5, 0.09375, ((0, 512),))
    w_key = bell_draw(arg_keys[4], (HEADS * DQK, D), D ** -0.5, 0.09375, ((0, 512),))
    w_value = bell_draw(arg_keys[5], (HEADS * DV, D), D ** -0.5, 0.09375, ((0, 512),))
    w_outgate = bell_draw(arg_keys[6], (HEADS * DV, D), D ** -0.5, 0.09375, ((0, 512),))
    w_input = bell_draw(arg_keys[7], (HEADS, D), D ** -0.5, 0.09375)
    w_forget = bell_draw(arg_keys[8], (HEADS, D), D ** -0.5, 0.09375)
    bias_input = bell_draw(arg_keys[9], (HEADS,), 1.0, 3.0, (), jnp.float32)
    bias_forget = jnp.clip(jax.random.uniform(arg_keys[10], (HEADS,), jnp.float32, -1.0, 4.0), -1.0, 4.0)
    w_read = bell_draw(arg_keys[11], (D, HEADS * DV), (HEADS * DV) ** -0.5, 0.125, ((0, 512),))
    cells = bell_draw(arg_keys[12], (HEADS * DV, DQK, BATCH), 0.25, 4.0, ((0, 512),), jnp.float32)
    norms = jnp.clip(jax.random.uniform(arg_keys[13], (HEADS * DQK, BATCH), jnp.float32, 0.0, 0.5), 0.0, 0.5)
    maxima = jnp.clip(jax.random.uniform(arg_keys[14], (HEADS, BATCH), jnp.float32, -1.0, 1.0), -1.0, 1.0)
    return {"tokens": tokens, "positions": positions, "norm_gain": norm_gain, "w_query": w_query, "w_key": w_key, "w_value": w_value, "w_outgate": w_outgate, "w_input": w_input, "w_forget": w_forget, "bias_input": bias_input, "bias_forget": bias_forget, "w_read": w_read, "cells": cells, "norms": norms, "maxima": maxima}


EPS = 1e-06

def reference(tokens, positions, norm_gain, w_query, w_key, w_value, w_outgate, w_input, w_forget, bias_input, bias_forget, w_read, cells, norms, maxima):
    where = positions.astype(jnp.float32)[None, :]
    wide = tokens.astype(jnp.float32)
    total = lax.optimization_barrier(jnp.sum(wide * wide, axis=0))
    scale = lax.rsqrt(total / D + EPS)[None, :]
    normed = (wide * norm_gain[:, None]).astype(jnp.bfloat16)
    query = (jnp.dot(w_query, normed, preferred_element_type=jnp.float32) * scale).astype(jnp.bfloat16)
    key = (jnp.dot(w_key, normed, preferred_element_type=jnp.float32) * scale * DQK ** (-0.5)).astype(jnp.bfloat16)
    value = jnp.dot(w_value, normed, preferred_element_type=jnp.float32) * scale
    outgate = jnp.dot(w_outgate, normed, preferred_element_type=jnp.float32) * scale
    gate_in = jnp.dot(w_input, normed, preferred_element_type=jnp.float32) * scale + bias_input[:, None]
    gate_forget = jnp.dot(w_forget, normed, preferred_element_type=jnp.float32) * scale + bias_forget[:, None]
    logf = jax.nn.log_sigmoid(gate_forget) * (1.0 + where / MOST_LEN)
    new_max = jnp.maximum(logf + maxima, gate_in)
    decay = jnp.exp(logf + maxima - new_max)
    fresh = jnp.exp(gate_in - new_max)
    head_cells, head_norms, head_out = ([], [], [])
    for head in range(HEADS):
        q_head = query[head * DQK:(head + 1) * DQK].astype(jnp.float32)
        k_head = key[head * DQK:(head + 1) * DQK].astype(jnp.float32)
        v_head = value[head * DV:(head + 1) * DV]
        c_old = cells[head * DV:(head + 1) * DV]
        n_old = norms[head * DQK:(head + 1) * DQK]
        c_new = decay[head][None, None, :] * c_old + fresh[head][None, None, :] * v_head[:, None, :] * k_head[None, :, :]
        n_new = decay[head][None, :] * n_old + fresh[head][None, :] * k_head
        denom = lax.optimization_barrier(jnp.sum(q_head * n_new, axis=0))
        numer = lax.optimization_barrier(jnp.sum(q_head[None, :, :] * c_new, axis=1))
        head_out.append(numer / jnp.maximum(jnp.abs(denom), 1.0)[None, :])
        head_cells.append(c_new)
        head_norms.append(n_new)
    hidden = jnp.concatenate(head_out, axis=0)
    gated = (hidden * jax.nn.sigmoid(outgate)).astype(jnp.bfloat16)
    mixed = jnp.dot(w_read, gated, preferred_element_type=jnp.float32)
    rows = (wide + mixed).astype(jnp.bfloat16)
    return (rows, jnp.concatenate(head_cells, axis=0), jnp.concatenate(head_norms, axis=0), new_max)
```

```python
import functools

import jax
import jax.numpy as jnp
from jax import lax
from jax.experimental import pallas as pl
from jax.experimental.pallas import tpu as pltpu
from jax.sharding import PartitionSpec as P

DQK = 256
MOST_LEN = 3072
EPS = 1e-06
NZ, NY, NX, NC = 16, 4, 4, 2
CUBE = 4
F32 = jnp.float32
BF16 = jnp.bfloat16
MESH = pl.DeviceIdType.MESH


def kernel(
    tokens,
    *refs,
):
    sources, (rows_out, cells_v, norms_v, max_out), rest = refs[:14], refs[14:18], refs[18:]
    held, rest = rest[:12], rest[12:]
    body(tokens, sources, held, rows_out, cells_v, norms_v, max_out, *rest)


def body(
    tokens,
    sources,
    held,
    rows_out,
    cells_v,
    norms_v,
    max_out,
    tok,
    gbuf,
    kq,
    weights,
    gain_b,
    qf,
    kf,
    dec,
    fre,
    local_sem,
    z_s,
    z_r,
    p1_s,
    p1_r,
    p2_s,
    p2_r,
    d_s,
    d_r,
    qz_s,
    qz_r,
    qy_s,
    qy_r,
    qx_s,
    qx_r,
    qd_s,
    qd_r,
):
    me = lax.axis_index("tp")
    core = me % NC
    x = (me // NC) % NX
    y = (me // (NC * NX)) % NY
    z = me // (NC * NX * NY)
    head = z // CUBE
    zlo = z % CUBE

    def device(zz, yy, xx, cc):
        return (((zz * NY + yy) * NX + xx) * NC + cc,)

    def send(ref, dst, ss, rs, to):
        return pltpu.make_async_remote_copy(
            src_ref=ref, dst_ref=dst, send_sem=ss, recv_sem=rs, device_id=to, device_id_type=MESH
        )

    loads = [
        pltpu.make_async_copy(
            tokens.at[:, pl.ds(128 * half, 128)], tok.at[half, z, y, x, core], local_sem.at[half]
        )
        for half in range(2)
    ]
    (where_ref, gain_ref, wq_ref, wk_ref, wv_ref, wo_ref, wi_ref, wf_ref) = held[:8]
    (bi_ref, bf_ref, wr_ref, maxima_ref) = held[8:]
    targets = held[:11] + (cells_v, norms_v, maxima_ref)
    for i, (source, target) in enumerate(zip(sources, targets)):
        loads.append(pltpu.make_async_copy(source, target, local_sem.at[2 + i]))
    for copy in loads:
        copy.start()

    barrier = pltpu.get_barrier_semaphore()

    def greet(to):
        pl.semaphore_signal(barrier, inc=1, device_id=to, device_id_type=MESH)

    @pl.loop(1, NZ)
    def _(dz):
        greet(device((z + dz) % NZ, y, x, core))

    @pl.loop(1, NY)
    def _(dy):
        greet(device(z, (y + dy) % NY, x, core))

    @pl.loop(1, NX)
    def _(dx):
        greet(device(z, y, (x + dx) % NX, core))

    greet(device(z, y, x, 1 - core))

    for i in (1, 2, 3, 4, 5, 6, 7):
        loads[2 + i].wait()

    weights[...] = jnp.zeros_like(weights)
    weights[0:2, :] = wq_ref[...]
    weights[2:4, :] = wk_ref[...]
    weights[4:8, :] = wv_ref[...]
    weights[8:12, :] = wo_ref[...]
    weights[12:16, :] = wi_ref[...]
    weights[16:20, :] = wf_ref[...]
    gain_t = gain_ref[...].T
    for r in range(2 * NZ):
        gain_b[r // 2, 128 * (r % 2) : 128 * (r % 2 + 1)] = jnp.broadcast_to(
            gain_t[:, r : r + 1], (128, 128)
        )

    pl.semaphore_wait(barrier, NZ - 1 + NY - 1 + NX - 1 + 1)
    for i in (0, 1, 2, 10, 11, 12, 15):
        loads[i].wait()

    def z_copy(buf, n, dz):
        mine = buf.at[:, z, y, x, core]
        return send(mine, mine, z_s.at[n, dz], z_r.at[n, dz], device((z + dz) % NZ, y, x, core))

    def first_copy(buf, n, half, d):
        mine = buf.at[half, :, y, x, core]
        to = device(z, (y + d) % NY, x, core) if half == 0 else device(z, y, (x + d) % NX, core)
        return send(mine, mine, p1_s.at[n, half, d], p1_r.at[n, half, d], to)

    def second_copy(buf, n, half, d):
        if half == 0:
            mine = buf.at[half, :, :, x, core]
            to = device(z, y, (x + d) % NX, core)
        else:
            mine = buf.at[half, :, y, :, core]
            to = device(z, (y + d) % NY, x, core)
        return send(mine, mine, p2_s.at[n, half, d], p2_r.at[n, half, d], to)

    def core_copy(buf, n, half, d):
        if half == 0:
            part = buf.at[half, :, :, (x + NX - d) % NX, core]
        else:
            part = buf.at[half, :, (y + NY - d) % NY, :, core]
        return send(part, part, d_s.at[n, half, d], d_r.at[n, half, d], device(z, y, x, 1 - core))

    def start_z(buf, n):
        @pl.loop(0, NZ - 1)
        def _(i):
            dz = 8 + ((i + 1) // 2) * (2 * (i % 2) - 1)
            z_copy(buf, n, dz).start()

    def finish_z(buf, n):
        @pl.loop(1, NZ)
        def _(dz):
            z_copy(buf, n, dz).wait_recv()

    def start_first(buf, n):
        for d in (2, 1, 3):
            for half in range(2):
                first_copy(buf, n, half, d).start()

    def second(buf, n):
        for half in range(2):
            for d in (1, 3, 2):
                first_copy(buf, n, half, d).wait_recv()
            for d in (2, 1, 3):
                second_copy(buf, n, half, d).start()
        for half in range(2):
            core_copy(buf, n, half, 0).start()
        for d in (1, 3, 2):
            for half in range(2):
                second_copy(buf, n, half, d).wait_recv()
                core_copy(buf, n, half, d).start()

    def finish_core(buf, n):
        for half in range(2):
            for d in range(4):
                core_copy(buf, n, half, d).wait_recv()

    def drain(buf, n):
        @pl.loop(1, NZ)
        def _(dz):
            z_copy(buf, n, dz).wait_send()

        for half in range(2):
            for d in range(1, 4):
                first_copy(buf, n, half, d).wait_send()
                second_copy(buf, n, half, d).wait_send()
            for d in range(4):
                core_copy(buf, n, half, d).wait_send()

    start_z(tok, 0)
    finish_z(tok, 0)
    start_first(tok, 0)
    second(tok, 0)
    finish_core(tok, 0)

    def project(i, carry):
        acc, squares = carry
        halves = []
        sums = []
        for half in range(2):
            t = tok[half, i].astype(F32).reshape(256, 128)
            sums.append(jnp.sum((t * t).reshape(32, 8, 128), axis=0))
            halves.append((t * gain_b[i]).astype(BF16))
        normed = jnp.concatenate(halves, axis=1)
        w = weights[:, pl.ds(pl.multiple_of(i * 256, 256), 256)]
        acc = acc + jnp.dot(w, normed, preferred_element_type=F32)
        return acc, squares + jnp.concatenate(sums, axis=1)

    acc, squares = lax.fori_loop(
        0, NZ, project, (jnp.zeros((32, 256), F32), jnp.zeros((8, 256), F32))
    )
    total = jnp.sum(squares, axis=0, keepdims=True)
    scale = lax.rsqrt(total / (NZ * NY * NX * NC * 8) + EPS)
    proj = acc * scale
    query = proj[0:2].astype(BF16)
    key = (proj[2:4] * DQK ** (-0.5)).astype(BF16)
    for half in range(2):
        kq[z, y, x, core, half] = key[:, 128 * half : 128 * (half + 1)]
        kq[z, y, x, core, 2 + half] = query[:, 128 * half : 128 * (half + 1)]

    def qz_copy(dz):
        mine = kq.at[z, y, x, core]
        to = device(head * CUBE + (zlo + dz) % CUBE, y, x, core)
        return send(mine, mine, qz_s.at[0, dz], qz_r.at[0, dz], to)

    def kz_copy(dh, j):
        mine = kq.at[z, y, x, core, pl.ds(0, 2)]
        to = device(((head + dh) % 4) * CUBE + (zlo + j) % CUBE, y, x, core)
        return send(mine, mine, qz_s.at[dh, j], qz_r.at[dh, j], to)

    def zs_of(dh):
        return pl.ds(((head + 4 - dh) % 4) * CUBE, CUBE)

    def parts(dh):
        return pl.ds(0, 4 if dh == 0 else 2)

    def qy_copy(dh, d):
        mine = kq.at[zs_of(dh), y, x, core, parts(dh)]
        to = device(z, (y + d) % NY, x, core)
        return send(mine, mine, qy_s.at[dh, d], qy_r.at[dh, d], to)

    def qx_copy(dh, d):
        mine = kq.at[zs_of(dh), :, x, core, parts(dh)]
        to = device(z, y, (x + d) % NX, core)
        return send(mine, mine, qx_s.at[dh, d], qx_r.at[dh, d], to)

    def qd_copy(dh, d):
        part = kq.at[zs_of(dh), :, (x + NX - d) % NX, core, parts(dh)]
        to = device(z, y, x, 1 - core)
        return send(part, part, qd_s.at[dh, d], qd_r.at[dh, d], to)

    for dz in (2, 1, 3):
        qz_copy(dz).start()
    for dh in (2, 1, 3):
        for j in range(CUBE):
            kz_copy(dh, j).start()

    value = proj[4:8]
    outgate = jax.nn.sigmoid(proj[8:12])
    length = 1.0 + where_ref[...].astype(F32) / MOST_LEN
    for h in range(4):
        gate_in = proj[12 + h : 13 + h] + bi_ref[h]
        forget = proj[16 + h : 17 + h] + bf_ref[h]
        logf = (jnp.minimum(forget, 0.0) - jnp.log1p(jnp.exp(-jnp.abs(forget)))) * length
        held = logf + maxima_ref[h : h + 1]
        new_max = jnp.maximum(held, gate_in)
        max_out[h : h + 1] = new_max
        dec[h] = jnp.exp(held - new_max)
        fre[h] = jnp.exp(gate_in - new_max)

    for dz in (1, 3, 2):
        qz_copy(dz).wait_recv()
    for d in (2, 1, 3):
        qy_copy(0, d).start()
    for d in (1, 3, 2):
        qy_copy(0, d).wait_recv()
    for d in (2, 1, 3):
        qx_copy(0, d).start()
    qd_copy(0, 0).start()
    for d in (1, 3, 2):
        qx_copy(0, d).wait_recv()
        qd_copy(0, d).start()
    for dh in range(1, 4):
        for j in range(CUBE):
            kz_copy(dh, j).wait_recv()
        for d in (2, 1, 3):
            qy_copy(dh, d).start()
    for d in range(4):
        qd_copy(0, d).wait_recv()

    for half in range(2):
        lanes = slice(128 * half, 128 * (half + 1))
        kf[:, lanes] = kq[zs_of(0), :, :, :, half].astype(F32).reshape(DQK, 128)
        qf[:, lanes] = kq[zs_of(0), :, :, :, 2 + half].astype(F32).reshape(DQK, 128)
    loads[13].wait()
    loads[14].wait()
    decay = dec[head]
    fresh = fre[head]
    fv = fresh * value

    def memory(i, carry):
        at = pl.ds(pl.multiple_of(i * 16, 16), 16)
        q, k = qf[at], kf[at]
        own = norms_v[pl.ds(pl.multiple_of(head * DQK + i * 16, 16), 16)]
        out = []
        for v in range(4):
            new = decay * cells_v[v, at] + fv[v : v + 1] * k
            cells_v[v, at] = new
            prod = q * new
            out.append(carry[v] + prod[0:8] + prod[8:16])
        prod = q * (decay * own + fresh * k)
        out.append(carry[4] + prod[0:8] + prod[8:16])
        return tuple(out)

    sums = lax.fori_loop(0, DQK // 16, memory, (jnp.zeros((8, 256), F32),) * 5)
    denom = jnp.sum(sums[4], axis=0, keepdims=True)
    numer = jnp.concatenate([jnp.sum(sums[v], axis=0, keepdims=True) for v in range(4)], axis=0)
    hidden = numer / jnp.maximum(jnp.abs(denom), 1.0)
    gated = (hidden * outgate).astype(BF16)
    for half in range(2):
        gbuf[half, z, y, x, core] = gated[:, 128 * half : 128 * (half + 1)]

    start_z(gbuf, 1)
    for dh in range(1, 4):
        for d in (1, 3, 2):
            qy_copy(dh, d).wait_recv()
        for d in (2, 1, 3):
            qx_copy(dh, d).start()
        qd_copy(dh, 0).start()
    finish_z(gbuf, 1)
    start_first(gbuf, 1)
    for dh in range(1, 4):
        for d in (1, 3, 2):
            qx_copy(dh, d).wait_recv()
            qd_copy(dh, d).start()
    second(gbuf, 1)

    for dh in range(1, 4):
        for d in range(4):
            qd_copy(dh, d).wait_recv()

    @pl.loop(0, 4)
    def _(h):
        rows = pl.ds(pl.multiple_of(h * DQK, DQK), DQK)
        for half in range(2):
            lanes = slice(128 * half, 128 * (half + 1))
            k = kq[pl.ds(h * CUBE, CUBE), :, :, :, half].astype(F32).reshape(DQK, 128)
            norms_v[rows, lanes] = dec[h][:, lanes] * norms_v[rows, lanes] + fre[h][:, lanes] * k

    finish_core(gbuf, 1)
    total_rows = NZ * NY * NX * NC * 4
    for half in range(2):
        g = gbuf[half].reshape(total_rows, 128)
        mixed = jnp.dot(wr_ref[...], g, preferred_element_type=F32)
        lanes = slice(128 * half, 128 * (half + 1))
        rows_out[:, lanes] = (tok[half, z, y, x, core].astype(F32) + mixed).astype(BF16)

    drain(tok, 0)
    drain(gbuf, 1)
    for dz in range(1, 4):
        qz_copy(dz).wait_send()
    for dh in range(1, 4):
        for j in range(CUBE):
            kz_copy(dh, j).wait_send()
    for dh in range(4):
        for d in range(1, 4):
            qy_copy(dh, d).wait_send()
            qx_copy(dh, d).wait_send()
        for d in range(4):
            qd_copy(dh, d).wait_send()


def step(
    tokens,
    positions,
    norm_gain,
    w_query,
    w_key,
    w_value,
    w_outgate,
    w_input,
    w_forget,
    bias_input,
    bias_forget,
    w_read,
    cells,
    norms,
    maxima,
):
    vmem = pl.BlockSpec(memory_space=pltpu.VMEM)
    dma = pltpu.SemaphoreType.DMA
    return pl.pallas_call(
        kernel,
        out_shape=(
            jax.ShapeDtypeStruct((8, 256), BF16),
            jax.ShapeDtypeStruct((4, 256, 256), F32),
            jax.ShapeDtypeStruct((1024, 256), F32),
            jax.ShapeDtypeStruct((4, 256), F32),
        ),
        in_specs=[pl.BlockSpec(memory_space=pltpu.HBM)] * 15,
        out_specs=(vmem,) * 4,
        scratch_shapes=[
            pltpu.VMEM((1, 256), jnp.int32),
            pltpu.VMEM((32, 128), F32),
            pltpu.VMEM((2, 4096), BF16),
            pltpu.VMEM((2, 4096), BF16),
            pltpu.VMEM((4, 4096), BF16),
            pltpu.VMEM((4, 4096), BF16),
            pltpu.VMEM((4, 4096), BF16),
            pltpu.VMEM((4, 4096), BF16),
            pltpu.SMEM((4,), F32),
            pltpu.SMEM((4,), F32),
            pltpu.VMEM((8, 2048), BF16),
            pltpu.VMEM((4, 256), F32),
            pltpu.VMEM((2, NZ, NY, NX, NC, 8, 128), BF16),
            pltpu.VMEM((2, NZ, NY, NX, NC, 4, 128), BF16),
            pltpu.VMEM((NZ, NY, NX, NC, 4, 2, 128), BF16),
            pltpu.VMEM((32, 4096), BF16),
            pltpu.VMEM((NZ, 256, 128), F32),
            pltpu.VMEM((256, 256), F32),
            pltpu.VMEM((256, 256), F32),
            pltpu.VMEM((4, 1, 256), F32),
            pltpu.VMEM((4, 1, 256), F32),
            dma((16,)),
            dma((2, 16)),
            dma((2, 16)),
            dma((2, 2, 4)),
            dma((2, 2, 4)),
            dma((2, 2, 4)),
            dma((2, 2, 4)),
            dma((2, 2, 4)),
            dma((2, 2, 4)),
            dma((4, 4)),
            dma((4, 4)),
            dma((4, 4)),
            dma((4, 4)),
            dma((4, 4)),
            dma((4, 4)),
            dma((4, 4)),
            dma((4, 4)),
        ],
        compiler_params=pltpu.CompilerParams(
            collective_id=0, has_side_effects=True, vmem_limit_bytes=64700000
        ),
    )(
        tokens,
        positions.reshape(1, 256),
        norm_gain.reshape(32, 128),
        w_query,
        w_key,
        w_value,
        w_outgate,
        w_input,
        w_forget,
        bias_input,
        bias_forget,
        w_read,
        cells,
        norms,
        maxima,
    )


def solution(mesh):
    return jax.shard_map(
        step,
        mesh=mesh,
        in_specs=(
            P("tp", None),
            P(),
            P(),
            P("tp", None),
            P("tp", None),
            P("tp", None),
            P("tp", None),
            P(),
            P(),
            P(),
            P(),
            P("tp", None),
            P("tp", None, None),
            P(),
            P(),
        ),
        out_specs=(P("tp", None), P("tp", None, None), P(), P()),
        check_vma=False,
    )
```

```python
import jax
import jax.numpy as jnp
from jax import lax
from jax.experimental import pallas as pl
from jax.experimental.pallas import tpu as pltpu
from jax.sharding import PartitionSpec as P

DQK = 256
MOST_LEN = 3072
EPS = 1e-06
NZ, NY, NX, NC = 16, 4, 4, 2
CUBE = 4
D = 4096
F32 = jnp.float32
BF16 = jnp.bfloat16
MESH = pl.DeviceIdType.MESH


def kernel(*refs):
    sources, (rows_out, cells_v, norms_v, max_out), rest = refs[:15], refs[15:19], refs[19:]
    held, rest = rest[:12], rest[12:]
    body(sources, held, rows_out, cells_v, norms_v, max_out, *rest)


def body(
    sources,
    held,
    rows_out,
    cells_v,
    norms_v,
    max_out,
    tok,
    slices,
    rslices,
    wgot,
    rgot,
    wgate,
    gain_b,
    part,
    got,
    rpart,
    rgots,
    gbuf,
    kq,
    qf,
    kf,
    dec,
    fre,
    local_sem,
    z_s,
    z_r,
    a_s,
    a_r,
    w_s,
    w_r,
    wr_s,
    wr_r,
    p_s,
    p_r,
    qz_s,
    qz_r,
    kz_s,
    kz_r,
    qy_s,
    qy_r,
    qx_s,
    qx_r,
    qd_s,
    qd_r,
):
    me = lax.axis_index("tp")
    core = me % NC
    x = (me // NC) % NX
    y = (me // (NC * NX)) % NY
    z = me // (NC * NX * NY)
    head = z // CUBE
    zlo = z % CUBE
    other = 1 - core
    a = x * other + y * core
    r = y * other + x * core

    def device(zz, yy, xx, cc):
        return (((zz * NY + yy) * NX + xx) * NC + cc,)

    def on_line(cls, t, cc):
        return device(z, t * (1 - cls) + y * cls, x * (1 - cls) + t * cls, cc)

    def send(ref, dst, ss, rs, to):
        return pltpu.make_async_remote_copy(
            src_ref=ref, dst_ref=dst, send_sem=ss, recv_sem=rs, device_id=to, device_id_type=MESH
        )

    (where_ref, gain_ref, wq_ref, wk_ref, wv_ref, wo_ref, wi_ref, wf_ref) = held[:8]
    (bi_ref, bf_ref, wr_ref, maxima_ref) = held[8:]
    targets = (tok.at[z, a],) + held[:11] + (cells_v, norms_v, maxima_ref)
    loads = [
        pltpu.make_async_copy(source, target, local_sem.at[i])
        for i, (source, target) in enumerate(zip(sources, targets))
    ]
    for copy in loads:
        copy.start()

    barrier = pltpu.get_barrier_semaphore()

    def greet(to):
        pl.semaphore_signal(barrier, inc=1, device_id=to, device_id_type=MESH)

    @pl.loop(0, NZ - 1)
    def _(i):
        dz = 8 + ((i + 1) // 2) * (2 * (i % 2) - 1)
        greet(device((z + dz) % NZ, y, x, core))

    for d in range(1, 4):
        for c in range(NC):
            greet(device(z, (y + d) % NY, x, c))
            greet(device(z, y, (x + d) % NX, c))
    greet(device(z, y, x, other))
    for dz in range(1, CUBE):
        for dy in range(1, NY):
            greet(device(head * CUBE + (zlo + dz) % CUBE, (y + dy) % NY, x, core))
    pl.semaphore_wait(barrier, NZ - 1 + 12 + 1 + 9)

    def z_copy(n, dz):
        mine = tok.at[z, a] if n == 0 else gbuf.at[:, z, a, core]
        return send(mine, mine, z_s.at[n, dz], z_r.at[n, dz], device((z + dz) % NZ, y, x, core))

    def a_copy(n, d):
        mine = tok.at[:, a] if n == 0 else gbuf.at[:, :, a, core]
        to = on_line(other, (a + d) % 4, core)
        return send(mine, mine, a_s.at[n, d], a_r.at[n, d], to)

    def start_z(n):
        @pl.loop(0, NZ - 1)
        def _(i):
            dz = 8 + ((i + 1) // 2) * (2 * (i % 2) - 1)
            z_copy(n, dz).start()

    def finish_z(n):
        @pl.loop(1, NZ)
        def _(dz):
            z_copy(n, dz).wait_recv()

    loads[0].wait()
    start_z(0)

    for i in (3, 4, 5, 6, 7, 8, 11):
        loads[i].wait()
    rows = jnp.concatenate(
        [
            wq_ref[...].astype(F32),
            wk_ref[...].astype(F32),
            wv_ref[...].astype(F32),
            wo_ref[...].astype(F32),
            jnp.zeros((4, D), F32),
            wi_ref[...].astype(F32),
            wf_ref[...].astype(F32),
        ],
        axis=0,
    )
    read = wr_ref[...].astype(F32)
    for t in range(4):
        for p in range(NZ // 2):
            at = slice(128 * p, 128 * (p + 1))
            zs = (2 * p, 2 * p + 1)
            by_y = jnp.concatenate(
                [rows[:, zz * 256 + t * 64 : zz * 256 + t * 64 + 64] for zz in zs], axis=1
            )
            by_x = jnp.concatenate(
                [
                    rows[:, zz * 256 + yy * 64 + t * 16 : zz * 256 + yy * 64 + t * 16 + 16]
                    for zz in zs
                    for yy in range(4)
                ],
                axis=1,
            )
            for cls, piece in ((0, by_y), (1, by_x)):
                slices[cls, t, :, at] = piece[0:16].astype(BF16)
                wgate[cls, t, :, at] = piece[16:24].astype(BF16)
        for p in range(NZ // 4):
            at = slice(128 * p, 128 * (p + 1))
            zs = range(4 * p, 4 * p + 4)
            rslices[0, t, :, at] = jnp.concatenate(
                [read[:, zz * 128 + t * 32 : zz * 128 + t * 32 + 32] for zz in zs], axis=1
            ).astype(BF16)
            rslices[1, t, :, at] = jnp.concatenate(
                [
                    read[:, zz * 128 + yy * 32 + t * 8 : zz * 128 + yy * 32 + t * 8 + 8]
                    for zz in zs
                    for yy in range(4)
                ],
                axis=1,
            ).astype(BF16)

    loads[2].wait()
    gain_t = gain_ref[...].T
    for zz in range(NZ):
        gain_lo = gain_t[:, 2 * zz : 2 * zz + 1]
        gain_hi = gain_t[:, 2 * zz + 1 : 2 * zz + 2]
        gain_b[zz, 0:128] = jnp.broadcast_to(gain_lo, (128, 128))
        gain_b[zz, 128:256] = jnp.broadcast_to(gain_hi, (128, 128))

    def w_copy(cls, d):
        mine = y * (1 - cls) + x * cls
        t = (mine + d) % 4
        return send(
            slices.at[cls, t],
            wgot.at[mine, core],
            w_s.at[cls, d],
            w_r.at[mine, core],
            on_line(cls, t, cls),
        )

    def r_copy(cls, d):
        mine = y * (1 - cls) + x * cls
        t = (mine + d) % 4
        return send(
            rslices.at[cls, t],
            rgot.at[mine, core],
            wr_s.at[cls, d],
            wr_r.at[mine, core],
            on_line(cls, t, cls),
        )

    w_copy(other, 0).start()
    for d in (2, 1, 3):
        w_copy(core, d).start()
        w_copy(other, d).start()
    r_copy(other, 0).start()
    for d in (2, 1, 3):
        r_copy(core, d).start()
        r_copy(other, d).start()
    wgot[r, core] = slices[core, r]
    rgot[r, core] = rslices[core, r]
    for half in range(2):
        gbuf[half, :, :, other] = jnp.zeros((NZ, 4, 4, 128), BF16)

    finish_z(0)
    for d in (2, 1, 3):
        a_copy(0, d).start()

    def got_weights(sem, ref):
        for d in range(4):
            t = (r + d) % 4
            if d > 0:
                send(ref.at[t, core], ref.at[t, core], sem.at[t, core], sem.at[t, core], device(z, y, x, other)).wait_recv()
            send(ref.at[t, other], ref.at[t, other], sem.at[t, other], sem.at[t, other], device(z, y, x, other)).wait_recv()

    got_weights(w_r, wgot)
    for d in (1, 3, 2):
        a_copy(0, d).wait_recv()

    acc = jnp.zeros((128, 256), F32)
    gates = jnp.zeros((8, 256), F32)
    squares = jnp.zeros((8, 256), F32)
    first = core == 0
    for p in range(4):
        blocks = []
        for zz in range(4 * p, 4 * p + 4):
            for aa in range(4):
                t = tok[zz, aa].astype(F32)
                squares = squares + t * t
                row = (y * other + aa * core) * 64 + (aa * other + x * core) * 16 + core * 8
                g = gain_b[zz, pl.ds(pl.multiple_of(row, 8), 8)]
                t = t * jnp.concatenate([g, g], axis=1)
                none = jnp.zeros_like(t)
                blocks.append(jnp.where(first, t, none))
                blocks.append(jnp.where(first, none, t))
        normed = jnp.concatenate(blocks, axis=0).astype(BF16)
        at = slice(256 * p, 256 * (p + 1))
        w = wgot[:, :, :, at].reshape(128, 256)
        acc = acc + jnp.dot(w, normed, preferred_element_type=F32)
        gates = gates + jnp.dot(wgate[core, r, :, at], normed, preferred_element_type=F32)
    total = jnp.sum(squares, axis=0, keepdims=True)
    for t in range(4):
        for c in range(NC):
            at = (t * 2 + c) * 16
            part[t, c, 0:16] = acc[at : at + 16]
            part[t, c, 16:24] = gates
            part[t, c, 12:13] = total

    def p_copy(n, c, d):
        t = (r + d) % 4
        source = part if n == 0 else rpart
        target = got if n == 0 else rgots
        return send(
            source.at[t, c], target.at[core, r], p_s.at[n, c, d], p_r.at[n, core, r], on_line(core, t, c)
        )

    def start_p(n):
        for d in (2, 1, 3):
            p_copy(n, core, d).start()
            p_copy(n, other, d).start()
        p_copy(n, other, 0).start()

    def finish_p(n):
        ref = got if n == 0 else rgots
        for d in range(4):
            t = (r + d) % 4
            if d > 0:
                mine = ref.at[core, t]
                send(mine, mine, p_r.at[n, core, t], p_r.at[n, core, t], device(z, y, x, other)).wait_recv()
            t = (a + d) % 4
            mine = ref.at[other, t]
            send(mine, mine, p_r.at[n, other, t], p_r.at[n, other, t], device(z, y, x, other)).wait_recv()

    start_p(0)
    got[core, r] = part[r, core]
    for i in (1, 9, 10, 14):
        loads[i].wait()
    length = 1.0 + where_ref[...].astype(F32) / MOST_LEN
    finish_p(0)
    sums = got[0, 0]
    for t in range(1, 8):
        sums = sums + got[t // 4, t % 4]
    scale = lax.rsqrt(sums[12:13] / D + EPS)
    proj = sums * scale
    query = proj[0:2].astype(BF16)
    key = (proj[2:4] * DQK ** (-0.5)).astype(BF16)
    for half in range(2):
        kq[z, y, x, core, half] = key[:, 128 * half : 128 * (half + 1)]
        kq[z, y, x, core, 2 + half] = query[:, 128 * half : 128 * (half + 1)]

    def qz_copy(dz, dy):
        mine = kq.at[z, y, x, core]
        to = device(head * CUBE + (zlo + dz) % CUBE, (y + dy) % NY, x, core)
        return send(mine, mine, qz_s.at[dz, dy], qz_r.at[dz, dy], to)

    def kz_copy(dh, j):
        mine = kq.at[z, y, x, core, pl.ds(0, 2)]
        to = device(((head + dh) % 4) * CUBE + (zlo + j) % CUBE, y, x, core)
        return send(mine, mine, kz_s.at[dh, j], kz_r.at[dh, j], to)

    def zs_of(dh):
        return pl.ds(((head + 4 - dh) % 4) * CUBE, CUBE)

    def parts(dh):
        return pl.ds(0, 4 if dh == 0 else 2)

    def qy_copy(dh, d):
        mine = kq.at[zs_of(dh), y, x, core, parts(dh)]
        to = device(z, (y + d) % NY, x, core)
        return send(mine, mine, qy_s.at[dh, d], qy_r.at[dh, d], to)

    def qx_copy(dh, d):
        mine = kq.at[zs_of(dh), :, x, core, parts(dh)]
        to = device(z, y, (x + d) % NX, core)
        return send(mine, mine, qx_s.at[dh, d], qx_r.at[dh, d], to)

    def qd_copy(dh, d):
        this = kq.at[zs_of(dh), :, (x + NX - d) % NX, core, parts(dh)]
        to = device(z, y, x, other)
        return send(this, this, qd_s.at[dh, d], qd_r.at[dh, d], to)

    near = [(dz, dy) for dz in range(4) for dy in range(4) if dz or dy]
    for dz, dy in sorted(near, key=lambda at: (-(at[0] > 1) - (at[1] == 2), at)):
        qz_copy(dz, dy).start()
    for dh in (2, 1, 3):
        for j in range(CUBE):
            kz_copy(dh, j).start()

    value = proj[4:8]
    outgate = jax.nn.sigmoid(proj[8:12])
    for h in range(4):
        gate_in = proj[16 + h : 17 + h] + bi_ref[h]
        forget = proj[20 + h : 21 + h] + bf_ref[h]
        logf = (jnp.minimum(forget, 0.0) - jnp.log1p(jnp.exp(-jnp.abs(forget)))) * length
        held_max = logf + maxima_ref[h : h + 1]
        new_max = jnp.maximum(held_max, gate_in)
        max_out[h : h + 1] = new_max
        dec[h] = jnp.exp(held_max - new_max)
        fre[h] = jnp.exp(gate_in - new_max)

    for dz, dy in near:
        qz_copy(dz, dy).wait_recv()
    for d in (2, 1, 3):
        qx_copy(0, d).start()
    qd_copy(0, 0).start()
    for d in (1, 3, 2):
        qx_copy(0, d).wait_recv()
        qd_copy(0, d).start()
    for dh in range(1, 4):
        for j in range(CUBE):
            kz_copy(dh, j).wait_recv()
        for d in (2, 1, 3):
            qy_copy(dh, d).start()
    for d in range(4):
        qd_copy(0, d).wait_recv()

    for half in range(2):
        lanes = slice(128 * half, 128 * (half + 1))
        kf[:, lanes] = kq[zs_of(0), :, :, :, half].astype(F32).reshape(DQK, 128)
        qf[:, lanes] = kq[zs_of(0), :, :, :, 2 + half].astype(F32).reshape(DQK, 128)
    loads[12].wait()
    loads[13].wait()
    decay = dec[head]
    fresh = fre[head]
    fv = fresh * value

    def memory(i, carry):
        at = pl.ds(pl.multiple_of(i * 16, 16), 16)
        q, k = qf[at], kf[at]
        own = norms_v[pl.ds(pl.multiple_of(head * DQK + i * 16, 16), 16)]
        out = []
        for v in range(4):
            new = decay * cells_v[v, at] + fv[v : v + 1] * k
            cells_v[v, at] = new
            prod = q * new
            out.append(carry[v] + prod[0:8] + prod[8:16])
        prod = q * (decay * own + fresh * k)
        out.append(carry[4] + prod[0:8] + prod[8:16])
        return tuple(out)

    sums = lax.fori_loop(0, DQK // 16, memory, (jnp.zeros((8, 256), F32),) * 5)
    denom = jnp.sum(sums[4], axis=0, keepdims=True)
    numer = jnp.concatenate([jnp.sum(sums[v], axis=0, keepdims=True) for v in range(4)], axis=0)
    hidden = numer / jnp.maximum(jnp.abs(denom), 1.0)
    gated = (hidden * outgate).astype(BF16)
    for half in range(2):
        gbuf[half, z, a, core] = gated[:, 128 * half : 128 * (half + 1)]

    start_z(1)
    got_weights(wr_r, rgot)
    for dh in range(1, 4):
        for d in (1, 3, 2):
            qy_copy(dh, d).wait_recv()
        for d in (2, 1, 3):
            qx_copy(dh, d).start()
        qd_copy(dh, 0).start()
    finish_z(1)
    for d in (2, 1, 3):
        a_copy(1, d).start()
    for dh in range(1, 4):
        for d in (1, 3, 2):
            qx_copy(dh, d).wait_recv()
            qd_copy(dh, d).start()
    for d in (1, 3, 2):
        a_copy(1, d).wait_recv()
    w = rgot[...].reshape(64, 512)
    for half in range(2):
        g = gbuf[half].reshape(512, 128)
        mixed = jnp.dot(w, g, preferred_element_type=F32)
        for t in range(4):
            for c in range(NC):
                at = (t * 2 + c) * 8
                rpart[t, c, :, 128 * half : 128 * (half + 1)] = mixed[at : at + 8]
    start_p(1)
    rgots[core, r] = rpart[r, core]

    for dh in range(1, 4):
        for d in range(4):
            qd_copy(dh, d).wait_recv()

    @pl.loop(0, 4)
    def _(h):
        at = pl.ds(pl.multiple_of(h * DQK, DQK), DQK)
        for half in range(2):
            lanes = slice(128 * half, 128 * (half + 1))
            k = kq[pl.ds(h * CUBE, CUBE), :, :, :, half].astype(F32).reshape(DQK, 128)
            norms_v[at, lanes] = dec[h][:, lanes] * norms_v[at, lanes] + fre[h][:, lanes] * k

    finish_p(1)
    mixed = rgots[0, 0]
    for t in range(1, 8):
        mixed = mixed + rgots[t // 4, t % 4]
    rows_out[...] = (tok[z, a].astype(F32) + mixed).astype(BF16)

    for n in range(2):

        @pl.loop(1, NZ)
        def _(dz):
            z_copy(n, dz).wait_send()

        for d in range(1, 4):
            a_copy(n, d).wait_send()
            p_copy(n, core, d).wait_send()
            p_copy(n, other, d).wait_send()
        p_copy(n, other, 0).wait_send()
    for copy in (w_copy, r_copy):
        copy(other, 0).wait_send()
        for d in range(1, 4):
            copy(core, d).wait_send()
            copy(other, d).wait_send()
    for dz, dy in near:
        qz_copy(dz, dy).wait_send()
    for dh in range(4):
        for d in range(1, 4):
            qx_copy(dh, d).wait_send()
        for d in range(4):
            qd_copy(dh, d).wait_send()
    for dh in range(1, 4):
        for j in range(CUBE):
            kz_copy(dh, j).wait_send()
        for d in range(1, 4):
            qy_copy(dh, d).wait_send()


def put(*refs):
    sems = refs[8]
    copies = [pltpu.make_async_copy(refs[i], refs[4 + i], sems.at[i]) for i in range(4)]
    for copy in copies:
        copy.start()
    for copy in copies:
        copy.wait()


RESULTS = (((8, 256), BF16), ((4, 256, 256), F32), ((1024, 256), F32), ((4, 256), F32))


def step(
    tokens,
    positions,
    norm_gain,
    w_query,
    w_key,
    w_value,
    w_outgate,
    w_input,
    w_forget,
    bias_input,
    bias_forget,
    w_read,
    cells,
    norms,
    maxima,
):
    vmem = pl.BlockSpec(memory_space=pltpu.VMEM)
    hbm = pl.BlockSpec(memory_space=pltpu.HBM)
    dma = pltpu.SemaphoreType.DMA
    operands = (
        tokens,
        positions.reshape(1, 256),
        norm_gain.reshape(32, 128),
        w_query,
        w_key,
        w_value,
        w_outgate,
        w_input,
        w_forget,
        bias_input,
        bias_forget,
        w_read,
        cells,
        norms,
        maxima,
    )
    results = pl.pallas_call(
        kernel,
        out_shape=tuple(pltpu.VMEM(shape, kind) for shape, kind in RESULTS),
        in_specs=[hbm] * 15,
        out_specs=(vmem,) * 4,
        scratch_shapes=[
            pltpu.VMEM((1, 256), jnp.int32),
            pltpu.VMEM((32, 128), F32),
            pltpu.VMEM((2, D), BF16),
            pltpu.VMEM((2, D), BF16),
            pltpu.VMEM((4, D), BF16),
            pltpu.VMEM((4, D), BF16),
            pltpu.VMEM((4, D), BF16),
            pltpu.VMEM((4, D), BF16),
            pltpu.SMEM((4,), F32),
            pltpu.SMEM((4,), F32),
            pltpu.VMEM((8, 2048), BF16),
            pltpu.VMEM((4, 256), F32),
            pltpu.VMEM((NZ, 4, 8, 256), BF16),
            pltpu.VMEM((2, 4, 16, 1024), BF16),
            pltpu.VMEM((2, 4, 8, 512), BF16),
            pltpu.VMEM((4, 2, 16, 1024), BF16),
            pltpu.VMEM((4, 2, 8, 512), BF16),
            pltpu.VMEM((2, 4, 8, 1024), BF16),
            pltpu.VMEM((NZ, 256, 128), F32),
            pltpu.VMEM((4, 2, 24, 256), F32),
            pltpu.VMEM((2, 4, 24, 256), F32),
            pltpu.VMEM((4, 2, 8, 256), F32),
            pltpu.VMEM((2, 4, 8, 256), F32),
            pltpu.VMEM((2, NZ, 4, 2, 4, 128), BF16),
            pltpu.VMEM((NZ, NY, NX, NC, 4, 2, 128), BF16),
            pltpu.VMEM((256, 256), F32),
            pltpu.VMEM((256, 256), F32),
            pltpu.VMEM((4, 1, 256), F32),
            pltpu.VMEM((4, 1, 256), F32),
            dma((15,)),
            dma((2, 16)),
            dma((2, 16)),
            dma((2, 4)),
            dma((2, 4)),
            dma((2, 4)),
            dma((4, 2)),
            dma((2, 4)),
            dma((4, 2)),
            dma((2, 2, 4)),
            dma((2, 2, 4)),
            dma((4, 4)),
            dma((4, 4)),
            dma((4, 4)),
            dma((4, 4)),
            dma((4, 4)),
            dma((4, 4)),
            dma((4, 4)),
            dma((4, 4)),
            dma((4, 4)),
            dma((4, 4)),
        ],
        compiler_params=pltpu.CompilerParams(
            collective_id=0, has_side_effects=True, vmem_limit_bytes=40 * 1024 * 1024
        ),
    )(*[pltpu.with_memory_space_constraint(operand, pltpu.HBM) for operand in operands])
    return pl.pallas_call(
        put,
        out_shape=tuple(pltpu.HBM(shape, kind) for shape, kind in RESULTS),
        in_specs=[vmem] * 4,
        out_specs=(hbm,) * 4,
        scratch_shapes=[dma((4,))],
    )(*[pltpu.with_memory_space_constraint(result, pltpu.VMEM) for result in results])


def solution(mesh):
    return jax.shard_map(
        step,
        mesh=mesh,
        in_specs=(
            P("tp", None),
            P(),
            P(),
            P("tp", None),
            P("tp", None),
            P("tp", None),
            P("tp", None),
            P(),
            P(),
            P(),
            P(),
            P("tp", None),
            P("tp", None, None),
            P(),
            P(),
        ),
        out_specs=(P("tp", None), P("tp", None, None), P(), P()),
        check_vma=False,
    )
```

```python
import jax
import jax.numpy as jnp
from jax import lax
from jax.experimental import pallas as pl
from jax.experimental.pallas import tpu as pltpu
from jax.sharding import PartitionSpec as P

DQK = 256
MOST_LEN = 3072
EPS = 1e-06
NZ, NY, NX, NC = 16, 4, 4, 2
CUBE = 4
D = 4096
F32 = jnp.float32
BF16 = jnp.bfloat16
MESH = pl.DeviceIdType.MESH


def kernel(*refs):
    sources, (rows_out, cells_v, norms_v, max_out), rest = refs[:15], refs[15:19], refs[19:]
    held, rest = rest[:12], rest[12:]
    body(sources, held, rows_out, cells_v, norms_v, max_out, *rest)


def body(
    sources,
    held,
    rows_out,
    cells_v,
    norms_v,
    max_out,
    tok,
    rows_v,
    slices,
    rslices,
    wgot,
    rgot,
    wgate,
    gain_b,
    part,
    got,
    lpart,
    lgot,
    rpart,
    rgots,
    gbuf,
    kq,
    qf,
    kf,
    dec,
    fre,
    local_sem,
    z_s,
    z_r,
    gz_s,
    gz_r,
    a_s,
    a_r,
    w_s,
    w_r,
    wr_s,
    wr_r,
    p_s,
    p_r,
    qz_s,
    qz_r,
    kz_s,
    kz_r,
    qy_s,
    qy_r,
    qx_s,
    qx_r,
    qd_s,
    qd_r,
):
    me = lax.axis_index("tp")
    core = me % NC
    x = (me // NC) % NX
    y = (me // (NC * NX)) % NY
    z = me // (NC * NX * NY)
    head = z // CUBE
    zlo = z % CUBE
    other = 1 - core
    a = x * other + y * core
    r = y * other + x * core

    def device(zz, yy, xx, cc):
        return (((zz * NY + yy) * NX + xx) * NC + cc,)

    def on_line(cls, t, cc):
        return device(z, t * (1 - cls) + y * cls, x * (1 - cls) + t * cls, cc)

    def send(ref, dst, ss, rs, to):
        return pltpu.make_async_remote_copy(
            src_ref=ref, dst_ref=dst, send_sem=ss, recv_sem=rs, device_id=to, device_id_type=MESH
        )

    (where_ref, gain_ref, wq_ref, wk_ref, wv_ref, wo_ref, wi_ref, wf_ref) = held[:8]
    (bi_ref, bf_ref, wr_ref, maxima_ref) = held[8:]
    targets = (tok.at[8, a],) + held[:11] + (cells_v, norms_v, maxima_ref)
    loads = [
        pltpu.make_async_copy(source, target, local_sem.at[i])
        for i, (source, target) in enumerate(zip(sources, targets))
    ]
    for copy in loads:
        copy.start()

    barrier = pltpu.get_barrier_semaphore()

    def greet(to):
        pl.semaphore_signal(barrier, inc=1, device_id=to, device_id_type=MESH)

    for dz in (4, -4, 3, -3, 2, -2, 1, -1):
        greet(device((z + NZ + dz) % NZ, y, x, core))
    for d in range(1, 4):
        for c in range(NC):
            greet(device(z, (y + d) % NY, x, c))
            greet(device(z, y, (x + d) % NX, c))
    greet(device(z, y, x, other))
    pl.semaphore_wait(barrier, 8 + 12 + 1)

    def near_copy(dz):
        to = device((z + NZ + dz) % NZ, y, x, core)
        return send(tok.at[8, a], tok.at[8 - dz, a], z_s.at[8 - dz], z_r.at[8 - dz], to)

    def far_copy(dz):
        source, target = (4, 4 - dz) if dz > 0 else (12, 12 - dz)
        to = device((z + NZ + dz) % NZ, y, x, core)
        return send(tok.at[source, a], tok.at[target, a], z_s.at[target], z_r.at[target], to)

    def a_copy(n, d):
        mine = tok.at[pl.ds((4, 0, 13)[n], (9, 4, 3)[n]), a]
        to = on_line(other, (a + d) % 4, core)
        return send(mine, mine, a_s.at[n, d], a_r.at[n, d], to)

    def gz_copy(dz):
        mine = gbuf.at[:, z, a, core]
        return send(mine, mine, gz_s.at[dz], gz_r.at[dz], device((z + dz) % NZ, y, x, core))

    def ga_copy(d):
        mine = gbuf.at[:, :, a, core]
        to = on_line(other, (a + d) % 4, core)
        return send(mine, mine, a_s.at[3, d], a_r.at[3, d], to)

    loads[0].wait()
    nearest = (4, -4, 3, -3, 2, -2, 1, -1)
    farther = (4, -3, 3, -2, 2, -1, 1)
    for dz in nearest:
        near_copy(dz).start()

    for i in (3, 4, 5, 6, 7, 8, 11):
        loads[i].wait()
    rows_v[...] = jnp.concatenate(
        [
            wq_ref[...].astype(F32),
            wk_ref[...].astype(F32),
            jnp.zeros((4, D), F32),
            wv_ref[...].astype(F32),
            wo_ref[...].astype(F32),
            wi_ref[...].astype(F32),
            wf_ref[...].astype(F32),
        ],
        axis=0,
    )
    read = wr_ref[...].astype(F32)
    for p in range(NZ // 2):
        at = slice(128 * p, 128 * (p + 1))
        pair = []
        for s in (2 * p, 2 * p + 1):
            zz = (z + s + 8) % NZ
            pair.append(rows_v[:, pl.ds(pl.multiple_of(zz * 256, 256), 256)])
        for t in range(4):
            by_y = jnp.concatenate([w[:, t * 64 : t * 64 + 64] for w in pair], axis=1)
            by_x = jnp.concatenate(
                [
                    w[:, yy * 64 + t * 16 : yy * 64 + t * 16 + 16]
                    for w in pair
                    for yy in range(4)
                ],
                axis=1,
            )
            for cls, piece in ((0, by_y), (1, by_x)):
                slices[cls, t, :, at] = piece[0:16].astype(BF16)
                wgate[cls, t, :, at] = piece[16:24].astype(BF16)
    for t in range(4):
        for p in range(NZ // 4):
            at = slice(128 * p, 128 * (p + 1))
            zs = range(4 * p, 4 * p + 4)
            rslices[0, t, :, at] = jnp.concatenate(
                [read[:, zz * 128 + t * 32 : zz * 128 + t * 32 + 32] for zz in zs], axis=1
            ).astype(BF16)
            rslices[1, t, :, at] = jnp.concatenate(
                [
                    read[:, zz * 128 + yy * 32 + t * 8 : zz * 128 + yy * 32 + t * 8 + 8]
                    for zz in zs
                    for yy in range(4)
                ],
                axis=1,
            ).astype(BF16)

    loads[2].wait()
    gain_t = gain_ref[...].T
    for zz in range(NZ):
        gain_lo = gain_t[:, 2 * zz : 2 * zz + 1]
        gain_hi = gain_t[:, 2 * zz + 1 : 2 * zz + 2]
        gain_b[zz, 0:128] = jnp.broadcast_to(gain_lo, (128, 128))
        gain_b[zz, 128:256] = jnp.broadcast_to(gain_hi, (128, 128))

    def w_copy(cls, d):
        mine = y * (1 - cls) + x * cls
        t = (mine + d) % 4
        return send(
            slices.at[cls, t],
            wgot.at[mine, core],
            w_s.at[cls, d],
            w_r.at[mine, core],
            on_line(cls, t, cls),
        )

    def r_copy(cls, d):
        mine = y * (1 - cls) + x * cls
        t = (mine + d) % 4
        return send(
            rslices.at[cls, t],
            rgot.at[mine, core],
            wr_s.at[cls, d],
            wr_r.at[mine, core],
            on_line(cls, t, cls),
        )

    w_copy(other, 0).start()
    for d in (2, 1, 3):
        w_copy(core, d).start()
        w_copy(other, d).start()
    r_copy(other, 0).start()
    for d in (2, 1, 3):
        r_copy(core, d).start()
        r_copy(other, d).start()
    wgot[r, core] = slices[core, r]
    rgot[r, core] = rslices[core, r]
    for half in range(2):
        gbuf[half, :, :, other] = jnp.zeros((NZ, 4, 4, 128), BF16)

    for dz in (4, -4):
        near_copy(dz).wait_recv()
    for dz in farther:
        far_copy(dz).start()
    for dz in (1, -1, 2, -2, 3, -3):
        near_copy(dz).wait_recv()
    for d in (2, 1, 3):
        a_copy(0, d).start()
    for dz in (1, 2, 3, 4):
        far_copy(dz).wait_recv()
    for d in (2, 1, 3):
        a_copy(1, d).start()
    for dz in (-1, -2, -3):
        far_copy(dz).wait_recv()
    for d in (2, 1, 3):
        a_copy(2, d).start()

    def got_weights(sem, ref):
        for d in range(4):
            t = (r + d) % 4
            if d > 0:
                send(ref.at[t, core], ref.at[t, core], sem.at[t, core], sem.at[t, core], device(z, y, x, other)).wait_recv()
            send(ref.at[t, other], ref.at[t, other], sem.at[t, other], sem.at[t, other], device(z, y, x, other)).wait_recv()

    got_weights(w_r, wgot)
    for n in range(3):
        for d in (1, 3, 2):
            a_copy(n, d).wait_recv()

    acc = jnp.zeros((128, 256), F32)
    gates = jnp.zeros((8, 256), F32)
    squares = jnp.zeros((8, 256), F32)
    first = core == 0
    for p in range(4):
        blocks = []
        for zz in range(4 * p, 4 * p + 4):
            for aa in range(4):
                t = tok[zz, aa].astype(F32)
                squares = squares + t * t
                row = (y * other + aa * core) * 64 + (aa * other + x * core) * 16 + core * 8
                g = gain_b[(z + zz + 8) % NZ, pl.ds(pl.multiple_of(row, 8), 8)]
                t = t * jnp.concatenate([g, g], axis=1)
                none = jnp.zeros_like(t)
                blocks.append(jnp.where(first, t, none))
                blocks.append(jnp.where(first, none, t))
        normed = jnp.concatenate(blocks, axis=0).astype(BF16)
        at = slice(256 * p, 256 * (p + 1))
        w = wgot[:, :, :, at].reshape(128, 256)
        acc = acc + jnp.dot(w, normed, preferred_element_type=F32)
        gates = gates + jnp.dot(wgate[core, r, :, at], normed, preferred_element_type=F32)
    total = jnp.sum(squares, axis=0, keepdims=True)
    for t in range(4):
        for c in range(NC):
            at = (t * 2 + c) * 16
            part[t, c, 0:4] = acc[at : at + 4]
            part[t, c, 4:5] = total

    def p_copy(n, c, d):
        t = (r + d) % 4
        source, target = ((part, got), (lpart, lgot), (rpart, rgots))[n]
        return send(
            source.at[t, c], target.at[core, r], p_s.at[n, c, d], p_r.at[n, core, r], on_line(core, t, c)
        )

    def start_p(n):
        for d in (2, 1, 3):
            p_copy(n, core, d).start()
            p_copy(n, other, d).start()
        p_copy(n, other, 0).start()

    def finish_p(n):
        ref = (got, lgot, rgots)[n]
        for d in range(4):
            t = (r + d) % 4
            if d > 0:
                mine = ref.at[core, t]
                send(mine, mine, p_r.at[n, core, t], p_r.at[n, core, t], device(z, y, x, other)).wait_recv()
            t = (a + d) % 4
            mine = ref.at[other, t]
            send(mine, mine, p_r.at[n, other, t], p_r.at[n, other, t], device(z, y, x, other)).wait_recv()

    start_p(0)
    for t in range(4):
        for c in range(NC):
            at = (t * 2 + c) * 16
            lpart[t, c, 0:8] = acc[at + 8 : at + 16]
            lpart[t, c, 8:16] = gates
    start_p(1)
    got[core, r] = part[r, core]
    lgot[core, r] = lpart[r, core]
    for i in (1, 9, 10, 14):
        loads[i].wait()
    length = 1.0 + where_ref[...].astype(F32) / MOST_LEN
    finish_p(0)
    sums = got[0, 0]
    for t in range(1, 8):
        sums = sums + got[t // 4, t % 4]
    scale = lax.rsqrt(sums[4:5] / D + EPS)
    proj = sums[0:4] * scale
    query = proj[0:2].astype(BF16)
    key = (proj[2:4] * DQK ** (-0.5)).astype(BF16)
    for half in range(2):
        kq[z, y, x, core, half] = key[:, 128 * half : 128 * (half + 1)]
        kq[z, y, x, core, 2 + half] = query[:, 128 * half : 128 * (half + 1)]

    def qz_copy(dz, dy):
        mine = kq.at[z, y, x, core]
        to = device(head * CUBE + (zlo + dz) % CUBE, (y + dy) % NY, x, core)
        return send(mine, mine, qz_s.at[dz, dy], qz_r.at[dz, dy], to)

    def kz_copy(dh, j):
        mine = kq.at[z, y, x, core, pl.ds(0, 2)]
        to = device(((head + dh) % 4) * CUBE + (zlo + j) % CUBE, y, x, core)
        return send(mine, mine, kz_s.at[dh, j], kz_r.at[dh, j], to)

    def zs_of(dh):
        return pl.ds(((head + 4 - dh) % 4) * CUBE, CUBE)

    def parts(dh):
        return pl.ds(0, 4 if dh == 0 else 2)

    def qy_copy(dh, d):
        mine = kq.at[zs_of(dh), y, x, core, parts(dh)]
        to = device(z, (y + d) % NY, x, core)
        return send(mine, mine, qy_s.at[dh, d], qy_r.at[dh, d], to)

    def qx_copy(dh, d):
        mine = kq.at[zs_of(dh), :, x, core, parts(dh)]
        to = device(z, y, (x + d) % NX, core)
        return send(mine, mine, qx_s.at[dh, d], qx_r.at[dh, d], to)

    def qd_copy(dh, d):
        this = kq.at[zs_of(dh), :, (x + NX - d) % NX, core, parts(dh)]
        to = device(z, y, x, other)
        return send(this, this, qd_s.at[dh, d], qd_r.at[dh, d], to)

    near = [(dz, dy) for dz in range(4) for dy in range(4) if dz or dy]
    for dz, dy in sorted(near, key=lambda at: (-(at[0] > 1) - (at[1] == 2), at)):
        qz_copy(dz, dy).start()
    for dh in (2, 1, 3):
        for j in range(CUBE):
            kz_copy(dh, j).start()

    finish_p(1)
    sums = lgot[0, 0]
    for t in range(1, 8):
        sums = sums + lgot[t // 4, t % 4]
    proj = sums * scale
    value = proj[0:4]
    outgate = jax.nn.sigmoid(proj[4:8])
    for h in range(4):
        gate_in = proj[8 + h : 9 + h] + bi_ref[h]
        forget = proj[12 + h : 13 + h] + bf_ref[h]
        logf = (jnp.minimum(forget, 0.0) - jnp.log1p(jnp.exp(-jnp.abs(forget)))) * length
        held_max = logf + maxima_ref[h : h + 1]
        new_max = jnp.maximum(held_max, gate_in)
        max_out[h : h + 1] = new_max
        dec[h] = jnp.exp(held_max - new_max)
        fre[h] = jnp.exp(gate_in - new_max)

    for dz, dy in near:
        qz_copy(dz, dy).wait_recv()
    for d in (2, 1, 3):
        qx_copy(0, d).start()
    qd_copy(0, 0).start()
    for d in (1, 3, 2):
        qx_copy(0, d).wait_recv()
        qd_copy(0, d).start()
    for dh in range(1, 4):
        for j in range(CUBE):
            kz_copy(dh, j).wait_recv()
        for d in (2, 1, 3):
            qy_copy(dh, d).start()
    for d in range(4):
        qd_copy(0, d).wait_recv()

    for half in range(2):
        lanes = slice(128 * half, 128 * (half + 1))
        kf[:, lanes] = kq[zs_of(0), :, :, :, half].astype(F32).reshape(DQK, 128)
        qf[:, lanes] = kq[zs_of(0), :, :, :, 2 + half].astype(F32).reshape(DQK, 128)
    loads[12].wait()
    loads[13].wait()
    decay = dec[head]
    fresh = fre[head]
    fv = fresh * value

    def memory(i, carry):
        at = pl.ds(pl.multiple_of(i * 16, 16), 16)
        q, k = qf[at], kf[at]
        own = norms_v[pl.ds(pl.multiple_of(head * DQK + i * 16, 16), 16)]
        out = []
        for v in range(4):
            new = decay * cells_v[v, at] + fv[v : v + 1] * k
            cells_v[v, at] = new
            prod = q * new
            out.append(carry[v] + prod[0:8] + prod[8:16])
        prod = q * (decay * own + fresh * k)
        out.append(carry[4] + prod[0:8] + prod[8:16])
        return tuple(out)

    sums = lax.fori_loop(0, DQK // 16, memory, (jnp.zeros((8, 256), F32),) * 5)
    denom = jnp.sum(sums[4], axis=0, keepdims=True)
    numer = jnp.concatenate([jnp.sum(sums[v], axis=0, keepdims=True) for v in range(4)], axis=0)
    hidden = numer / jnp.maximum(jnp.abs(denom), 1.0)
    gated = (hidden * outgate).astype(BF16)
    for half in range(2):
        gbuf[half, z, a, core] = gated[:, 128 * half : 128 * (half + 1)]

    for i in range(NZ - 1):
        gz_copy(8 + ((i + 1) // 2) * (2 * (i % 2) - 1)).start()
    got_weights(wr_r, rgot)
    for dh in range(1, 4):
        for d in (1, 3, 2):
            qy_copy(dh, d).wait_recv()
        for d in (2, 1, 3):
            qx_copy(dh, d).start()
        qd_copy(dh, 0).start()
    for dz in range(1, NZ):
        gz_copy(dz).wait_recv()
    for d in (2, 1, 3):
        ga_copy(d).start()
    for dh in range(1, 4):
        for d in (1, 3, 2):
            qx_copy(dh, d).wait_recv()
            qd_copy(dh, d).start()
    for d in (1, 3, 2):
        ga_copy(d).wait_recv()
    w = rgot[...].reshape(64, 512)
    for half in range(2):
        g = gbuf[half].reshape(512, 128)
        mixed = jnp.dot(w, g, preferred_element_type=F32)
        for t in range(4):
            for c in range(NC):
                at = (t * 2 + c) * 8
                rpart[t, c, :, 128 * half : 128 * (half + 1)] = mixed[at : at + 8]
    start_p(2)
    rgots[core, r] = rpart[r, core]

    for dh in range(1, 4):
        for d in range(4):
            qd_copy(dh, d).wait_recv()

    @pl.loop(0, 4)
    def _(h):
        at = pl.ds(pl.multiple_of(h * DQK, DQK), DQK)
        for half in range(2):
            lanes = slice(128 * half, 128 * (half + 1))
            k = kq[pl.ds(h * CUBE, CUBE), :, :, :, half].astype(F32).reshape(DQK, 128)
            norms_v[at, lanes] = dec[h][:, lanes] * norms_v[at, lanes] + fre[h][:, lanes] * k

    finish_p(2)
    mixed = rgots[0, 0]
    for t in range(1, 8):
        mixed = mixed + rgots[t // 4, t % 4]
    rows_out[...] = (tok[8, a].astype(F32) + mixed).astype(BF16)

    for dz in nearest:
        near_copy(dz).wait_send()
    for dz in farther:
        far_copy(dz).wait_send()
    for dz in range(1, NZ):
        gz_copy(dz).wait_send()
    for d in range(1, 4):
        ga_copy(d).wait_send()
    for n in range(3):
        for d in range(1, 4):
            a_copy(n, d).wait_send()
            p_copy(n, core, d).wait_send()
            p_copy(n, other, d).wait_send()
        p_copy(n, other, 0).wait_send()
    for copy in (w_copy, r_copy):
        copy(other, 0).wait_send()
        for d in range(1, 4):
            copy(core, d).wait_send()
            copy(other, d).wait_send()
    for dz, dy in near:
        qz_copy(dz, dy).wait_send()
    for dh in range(4):
        for d in range(1, 4):
            qx_copy(dh, d).wait_send()
        for d in range(4):
            qd_copy(dh, d).wait_send()
    for dh in range(1, 4):
        for j in range(CUBE):
            kz_copy(dh, j).wait_send()
        for d in range(1, 4):
            qy_copy(dh, d).wait_send()


def put(*refs):
    sems = refs[8]
    copies = [pltpu.make_async_copy(refs[i], refs[4 + i], sems.at[i]) for i in range(4)]
    for copy in copies:
        copy.start()
    for copy in copies:
        copy.wait()


RESULTS = (((8, 256), BF16), ((4, 256, 256), F32), ((1024, 256), F32), ((4, 256), F32))


def step(
    tokens,
    positions,
    norm_gain,
    w_query,
    w_key,
    w_value,
    w_outgate,
    w_input,
    w_forget,
    bias_input,
    bias_forget,
    w_read,
    cells,
    norms,
    maxima,
):
    vmem = pl.BlockSpec(memory_space=pltpu.VMEM)
    hbm = pl.BlockSpec(memory_space=pltpu.HBM)
    dma = pltpu.SemaphoreType.DMA
    operands = (
        tokens,
        positions.reshape(1, 256),
        norm_gain.reshape(32, 128),
        w_query,
        w_key,
        w_value,
        w_outgate,
        w_input,
        w_forget,
        bias_input,
        bias_forget,
        w_read,
        cells,
        norms,
        maxima,
    )
    results = pl.pallas_call(
        kernel,
        out_shape=tuple(pltpu.VMEM(shape, kind) for shape, kind in RESULTS),
        in_specs=[hbm] * 15,
        out_specs=(vmem,) * 4,
        scratch_shapes=[
            pltpu.VMEM((1, 256), jnp.int32),
            pltpu.VMEM((32, 128), F32),
            pltpu.VMEM((2, D), BF16),
            pltpu.VMEM((2, D), BF16),
            pltpu.VMEM((4, D), BF16),
            pltpu.VMEM((4, D), BF16),
            pltpu.VMEM((4, D), BF16),
            pltpu.VMEM((4, D), BF16),
            pltpu.SMEM((4,), F32),
            pltpu.SMEM((4,), F32),
            pltpu.VMEM((8, 2048), BF16),
            pltpu.VMEM((4, 256), F32),
            pltpu.VMEM((NZ, 4, 8, 256), BF16),
            pltpu.VMEM((24, D), F32),
            pltpu.VMEM((2, 4, 16, 1024), BF16),
            pltpu.VMEM((2, 4, 8, 512), BF16),
            pltpu.VMEM((4, 2, 16, 1024), BF16),
            pltpu.VMEM((4, 2, 8, 512), BF16),
            pltpu.VMEM((2, 4, 8, 1024), BF16),
            pltpu.VMEM((NZ, 256, 128), F32),
            pltpu.VMEM((4, 2, 8, 256), F32),
            pltpu.VMEM((2, 4, 8, 256), F32),
            pltpu.VMEM((4, 2, 16, 256), F32),
            pltpu.VMEM((2, 4, 16, 256), F32),
            pltpu.VMEM((4, 2, 8, 256), F32),
            pltpu.VMEM((2, 4, 8, 256), F32),
            pltpu.VMEM((2, NZ, 4, 2, 4, 128), BF16),
            pltpu.VMEM((NZ, NY, NX, NC, 4, 2, 128), BF16),
            pltpu.VMEM((256, 256), F32),
            pltpu.VMEM((256, 256), F32),
            pltpu.VMEM((4, 1, 256), F32),
            pltpu.VMEM((4, 1, 256), F32),
            dma((15,)),
            dma((16,)),
            dma((16,)),
            dma((16,)),
            dma((16,)),
            dma((4, 4)),
            dma((4, 4)),
            dma((2, 4)),
            dma((4, 2)),
            dma((2, 4)),
            dma((4, 2)),
            dma((3, 2, 4)),
            dma((3, 2, 4)),
            dma((4, 4)),
            dma((4, 4)),
            dma((4, 4)),
            dma((4, 4)),
            dma((4, 4)),
            dma((4, 4)),
            dma((4, 4)),
            dma((4, 4)),
            dma((4, 4)),
            dma((4, 4)),
        ],
        compiler_params=pltpu.CompilerParams(
            collective_id=0, has_side_effects=True, vmem_limit_bytes=40 * 1024 * 1024
        ),
    )(*[pltpu.with_memory_space_constraint(operand, pltpu.HBM) for operand in operands])
    return pl.pallas_call(
        put,
        out_shape=tuple(pltpu.HBM(shape, kind) for shape, kind in RESULTS),
        in_specs=[vmem] * 4,
        out_specs=(hbm,) * 4,
        scratch_shapes=[dma((4,))],
    )(*[pltpu.with_memory_space_constraint(result, pltpu.VMEM) for result in results])


def solution(mesh):
    return jax.shard_map(
        step,
        mesh=mesh,
        in_specs=(
            P("tp", None),
            P(),
            P(),
            P("tp", None),
            P("tp", None),
            P("tp", None),
            P("tp", None),
            P(),
            P(),
            P(),
            P(),
            P("tp", None),
            P("tp", None, None),
            P(),
            P(),
        ),
        out_specs=(P("tp", None), P("tp", None, None), P(), P()),
        check_vma=False,
    )
```

```python
import jax
import jax.numpy as jnp
from jax import lax
from jax.experimental import pallas as pl
from jax.experimental.pallas import tpu as pltpu
from jax.sharding import PartitionSpec as P

DQK = 256
MOST_LEN = 3072
EPS = 1e-06
NZ, NY, NX, NC = 16, 4, 4, 2
CUBE = 4
D = 4096
F32 = jnp.float32
BF16 = jnp.bfloat16
MESH = pl.DeviceIdType.MESH


def kernel(*refs):
    sources, (rows_out, cells_v, norms_v, max_out), rest = refs[:15], refs[15:19], refs[19:]
    held, rest = rest[:12], rest[12:]
    body(sources, held, rows_out, cells_v, norms_v, max_out, *rest)


def body(
    sources,
    held,
    rows_out,
    cells_v,
    norms_v,
    max_out,
    tok,
    rows_v,
    slices,
    rslices,
    wgot,
    rgot,
    wgate,
    gain_b,
    part,
    got,
    lpart,
    lgot,
    rpart,
    rgots,
    gbuf,
    kq,
    dec,
    fre,
    local_sem,
    z_s,
    z_r,
    a_s,
    a_r,
    w_s,
    w_r,
    p_s,
    p_r,
    q_s,
    q_r,
    qx_r,
):
    me = lax.axis_index("tp")
    core = me % NC
    x = (me // NC) % NX
    y = (me // (NC * NX)) % NY
    z = me // (NC * NX * NY)
    head = z // CUBE
    zlo = z % CUBE
    other = 1 - core
    a = x * other + y * core
    r = y * other + x * core

    def device(zz, yy, xx, cc):
        return (((zz * NY + yy) * NX + xx) * NC + cc,)

    def on_line(cls, t, cc):
        return device(z, t * (1 - cls) + y * cls, x * (1 - cls) + t * cls, cc)

    def send(ref, dst, ss, rs, to):
        return pltpu.make_async_remote_copy(
            src_ref=ref, dst_ref=dst, send_sem=ss, recv_sem=rs, device_id=to, device_id_type=MESH
        )

    (where_ref, gain_ref, wq_ref, wk_ref, wv_ref, wo_ref, wi_ref, wf_ref) = held[:8]
    (bi_ref, bf_ref, wr_ref, maxima_ref) = held[8:]
    targets = (tok.at[8, a],) + held[:11] + (cells_v, norms_v, maxima_ref)
    groups = (0, 2, 1, 1, 1, 1, 1, 1, 1, 3, 4, 1, 5, 6, 7)
    for source, target, group in zip(sources, targets, groups):
        pltpu.make_async_copy(source, target, local_sem.at[group]).start()

    def loaded(i, ref=None):
        target = targets[i] if ref is None else ref
        pltpu.make_async_copy(target, target, local_sem.at[groups[i]]).wait()

    partner = device(z, y, x, other)

    def arrived(sem, ref):
        send(ref, ref, sem, sem, partner).wait_recv()

    def left(sem, ref):
        send(ref, ref, sem, sem, partner).wait_send()

    barrier = pltpu.get_barrier_semaphore()

    def greet(to):
        pl.semaphore_signal(barrier, inc=1, device_id=to, device_id_type=MESH)

    for dz in (4, -4, 3, -3, 2, -2, 1, -1):
        greet(device((z + NZ + dz) % NZ, y, x, core))
    for d in range(1, 4):
        for c in range(NC):
            greet(device(z, (y + d) % NY, x, c))
            greet(device(z, y, (x + d) % NX, c))
    greet(partner)
    pl.semaphore_wait(barrier, 8 + 12 + 1)

    def near_copy(dz):
        to = device((z + NZ + dz) % NZ, y, x, core)
        group = 0 if dz == 4 else 1 if dz == -4 else 2
        return send(tok.at[8, a], tok.at[8 - dz, a], z_s.at[0], z_r.at[group], to)

    def far_copy(dz):
        source, target, group = (4, 4 - dz, 3) if dz > 0 else (12, 12 - dz, 4)
        to = device((z + NZ + dz) % NZ, y, x, core)
        return send(tok.at[source, a], tok.at[target, a], z_s.at[0], z_r.at[group], to)

    def a_copy(n, d):
        mine = tok.at[pl.ds((4, 0, 13)[n], (9, 4, 3)[n]), a]
        to = on_line(other, (a + d) % 4, core)
        return send(mine, mine, a_s.at[0], a_r.at[0], to)

    def gz_copy(dz):
        mine = gbuf.at[:, z, a, core]
        return send(mine, mine, z_s.at[1], z_r.at[5], device((z + dz) % NZ, y, x, core))

    def ga_copy(d):
        mine = gbuf.at[:, :, a, core]
        to = on_line(other, (a + d) % 4, core)
        return send(mine, mine, a_s.at[1], a_r.at[1], to)

    loaded(0)
    nearest = (4, -4, 3, -3, 2, -2, 1, -1)
    farther = (4, -3, 3, -2, 2, -1, 1)
    for dz in nearest:
        near_copy(dz).start()

    loaded(2, gain_b.at[pl.ds(0, 13), pl.ds(0, 32)])
    rows_v[...] = jnp.concatenate(
        [
            wq_ref[...].astype(F32),
            wk_ref[...].astype(F32),
            jnp.zeros((4, D), F32),
            wv_ref[...].astype(F32),
            wo_ref[...].astype(F32),
            wi_ref[...].astype(F32),
            wf_ref[...].astype(F32),
        ],
        axis=0,
    )
    read = wr_ref[...].astype(F32)
    for p in range(NZ // 2):
        at = slice(128 * p, 128 * (p + 1))
        pair = []
        for s in (2 * p, 2 * p + 1):
            zz = (z + s + 8) % NZ
            pair.append(rows_v[:, pl.ds(pl.multiple_of(zz * 256, 256), 256)])
        for t in range(4):
            by_y = jnp.concatenate([w[:, t * 64 : t * 64 + 64] for w in pair], axis=1)
            by_x = jnp.concatenate(
                [
                    w[:, yy * 64 + t * 16 : yy * 64 + t * 16 + 16]
                    for w in pair
                    for yy in range(4)
                ],
                axis=1,
            )
            for cls, piece in ((0, by_y), (1, by_x)):
                slices[cls * 4 + t, :, at] = piece[0:16].astype(BF16)
                wgate[cls * 4 + t, :, at] = piece[16:24].astype(BF16)
    for t in range(4):
        for p in range(NZ // 4):
            at = slice(128 * p, 128 * (p + 1))
            zs = range(4 * p, 4 * p + 4)
            rslices[t, :, at] = jnp.concatenate(
                [read[:, zz * 128 + t * 32 : zz * 128 + t * 32 + 32] for zz in zs], axis=1
            ).astype(BF16)
            rslices[4 + t, :, at] = jnp.concatenate(
                [
                    read[:, zz * 128 + yy * 32 + t * 8 : zz * 128 + yy * 32 + t * 8 + 8]
                    for zz in zs
                    for yy in range(4)
                ],
                axis=1,
            ).astype(BF16)

    gain_t = gain_ref[...].T
    for zz in range(NZ):
        gain_lo = gain_t[:, 2 * zz : 2 * zz + 1]
        gain_hi = gain_t[:, 2 * zz + 1 : 2 * zz + 2]
        gain_b[zz, 0:128] = jnp.broadcast_to(gain_lo, (128, 128))
        gain_b[zz, 128:256] = jnp.broadcast_to(gain_hi, (128, 128))

    def w_copy(cls, d):
        mine = y * (1 - cls) + x * cls
        t = (mine + d) % 4
        to = on_line(cls, t, cls)
        return send(
            slices.at[cls * 4 + t], wgot.at[mine * 2 + core], w_s.at[0], w_r.at[0], to
        )

    def r_copy(cls, d):
        mine = y * (1 - cls) + x * cls
        t = (mine + d) % 4
        to = on_line(cls, t, cls)
        return send(
            rslices.at[cls * 4 + t], rgot.at[mine * 2 + core], w_s.at[1], w_r.at[1], to
        )

    w_copy(other, 0).start()
    for d in (2, 1, 3):
        w_copy(core, d).start()
        w_copy(other, d).start()
    r_copy(other, 0).start()
    for d in (2, 1, 3):
        r_copy(core, d).start()
        r_copy(other, d).start()
    wgot[r * 2 + core] = slices[core * 4 + r]
    rgot[r * 2 + core] = rslices[core * 4 + r]
    for half in range(2):
        gbuf[half, :, :, other] = jnp.zeros((NZ, 4, 4, 128), BF16)

    arrived(z_r.at[0], tok.at[4, a])
    arrived(z_r.at[1], tok.at[12, a])
    for dz in farther:
        far_copy(dz).start()
    arrived(z_r.at[2], tok.at[pl.ds(5, 6), a])
    for d in (2, 1, 3):
        a_copy(0, d).start()
    arrived(z_r.at[3], tok.at[pl.ds(0, 4), a])
    for d in (2, 1, 3):
        a_copy(1, d).start()
    arrived(z_r.at[4], tok.at[pl.ds(13, 3), a])
    for d in (2, 1, 3):
        a_copy(2, d).start()

    arrived(w_r.at[0], wgot.at[pl.ds(0, 7)])
    arrived(a_r.at[0], tok.at[:, pl.ds(0, 3)])

    acc = jnp.zeros((128, 256), F32)
    gates = jnp.zeros((8, 256), F32)
    squares = jnp.zeros((8, 256), F32)
    first = core == 0
    for p in range(4):
        blocks = []
        for zz in range(4 * p, 4 * p + 4):
            for aa in range(4):
                t = tok[zz, aa].astype(F32)
                squares = squares + t * t
                row = (y * other + aa * core) * 64 + (aa * other + x * core) * 16 + core * 8
                g = gain_b[(z + zz + 8) % NZ, pl.ds(pl.multiple_of(row, 8), 8)]
                t = t * jnp.concatenate([g, g], axis=1)
                none = jnp.zeros_like(t)
                blocks.append(jnp.where(first, t, none))
                blocks.append(jnp.where(first, none, t))
        normed = jnp.concatenate(blocks, axis=0).astype(BF16)
        at = slice(256 * p, 256 * (p + 1))
        w = wgot[:, :, at].reshape(128, 256)
        acc = acc + jnp.dot(w, normed, preferred_element_type=F32)
        gates = gates + jnp.dot(wgate[core * 4 + r, :, at], normed, preferred_element_type=F32)
    total = jnp.sum(squares, axis=0, keepdims=True)
    for t in range(4):
        for c in range(NC):
            at = (t * 2 + c) * 16
            part[t * 2 + c, 0:4] = acc[at : at + 4]
            part[t * 2 + c, 4:5] = total

    def p_copy(n, c, d):
        t = (r + d) % 4
        source, target = ((part, got), (lpart, lgot), (rpart, rgots))[n]
        to = on_line(core, t, c)
        return send(source.at[t * 2 + c], target.at[core * 4 + r], p_s.at[n], p_r.at[n], to)

    def start_p(n):
        for d in (2, 1, 3):
            p_copy(n, core, d).start()
            p_copy(n, other, d).start()
        p_copy(n, other, 0).start()

    def finish_p(n):
        arrived(p_r.at[n], (got, lgot, rgots)[n].at[pl.ds(0, 7)])

    start_p(0)
    for t in range(4):
        for c in range(NC):
            at = (t * 2 + c) * 16
            lpart[t * 2 + c, 0:8] = acc[at + 8 : at + 16]
            lpart[t * 2 + c, 8:16] = gates
    start_p(1)
    got[core * 4 + r] = part[r * 2 + core]
    lgot[core * 4 + r] = lpart[r * 2 + core]
    for i in (1, 9, 10, 14):
        loaded(i)
    length = 1.0 + where_ref[...].astype(F32) / MOST_LEN
    finish_p(0)
    sums = got[0]
    for t in range(1, 8):
        sums = sums + got[t]
    scale = lax.rsqrt(sums[4:5] / D + EPS)
    proj = sums[0:4] * scale
    query = proj[0:2].astype(BF16)
    key = (proj[2:4] * DQK ** (-0.5)).astype(BF16)
    for half in range(2):
        kq[core, z, r, a, half] = key[:, 128 * half : 128 * (half + 1)]
        kq[core, z, r, a, 2 + half] = query[:, 128 * half : 128 * (half + 1)]

    def place(zz, tr, ta):
        return device(zz, tr * other + ta * core, ta * other + tr * core, core)

    def zs_of(dh):
        return pl.ds(((head + 4 - dh) % 4) * CUBE, CUBE)

    def parts(dh):
        return pl.ds(0, 4 if dh == 0 else 2)

    def qz_copy(dz, dr):
        mine = kq.at[core, z, r, a]
        to = place(head * CUBE + (zlo + dz) % CUBE, (r + dr) % 4, a)
        return send(mine, mine, q_s.at[0], q_r.at[0], to)

    def kz_copy(dh, j):
        mine = kq.at[core, z, r, a, pl.ds(0, 2)]
        to = place(((head + dh) % 4) * CUBE + (zlo + j) % CUBE, r, a)
        return send(mine, mine, q_s.at[1], q_r.at[1], to)

    def qy_copy(dh, d):
        mine = kq.at[core, zs_of(dh), r, a, parts(dh)]
        return send(mine, mine, q_s.at[2], q_r.at[2], place(z, (r + d) % 4, a))

    def qx_copy(dh, d):
        mine = kq.at[core, zs_of(dh), :, a, parts(dh)]
        if dh == 0:
            ss, rs = q_s.at[3], qx_r.at[d]
        else:
            ss, rs = q_s.at[4], q_r.at[4]
        return send(mine, mine, ss, rs, place(z, r, (a + d) % 4))

    def qd_copy(dh, d):
        this = kq.at[core, zs_of(dh), :, (a + 4 - d) % 4, parts(dh)]
        n = 5 if dh == 0 else 6
        return send(this, this, q_s.at[n], q_r.at[n], partner)

    def some(n):
        return (
            kq.at[0, pl.ds(0, 15), 0, 0],
            kq.at[0, pl.ds(0, 12), 0, 0, pl.ds(0, 2)],
            kq.at[0, pl.ds(0, 9), :, 0, pl.ds(0, 2)],
            kq.at[0, pl.ds(0, 12), :, 0],
            kq.at[0, pl.ds(0, 9), :, :, pl.ds(0, 2)],
            kq.at[0, :, :, 0],
            kq.at[0, pl.ds(0, 12), :, :, pl.ds(0, 2)],
        )[n]

    near = [(dz, dy) for dz in range(4) for dy in range(4) if dz or dy]
    for dz, dy in sorted(near, key=lambda at: (-(at[0] > 1) - (at[1] == 2), at)):
        qz_copy(dz, dy).start()
    for dh in (2, 1, 3):
        for j in range(CUBE):
            kz_copy(dh, j).start()

    finish_p(1)
    sums = lgot[0]
    for t in range(1, 8):
        sums = sums + lgot[t]
    proj = sums * scale
    value = proj[0:4]
    outgate = jax.nn.sigmoid(proj[4:8])
    for h in range(4):
        gate_in = proj[8 + h : 9 + h] + bi_ref[h]
        forget = proj[12 + h : 13 + h] + bf_ref[h]
        logf = (jnp.minimum(forget, 0.0) - jnp.log1p(jnp.exp(-jnp.abs(forget)))) * length
        held_max = logf + maxima_ref[h : h + 1]
        new_max = jnp.maximum(held_max, gate_in)
        max_out[h : h + 1] = new_max
        dec[h] = jnp.exp(held_max - new_max)
        fre[h] = jnp.exp(gate_in - new_max)

    arrived(q_r.at[0], some(0))
    for d in (2, 1, 3):
        qx_copy(0, d).start()
    qd_copy(0, 0).start()
    for d in (1, 3, 2):
        qx_copy(0, d).wait_recv()
        qd_copy(0, d).start()
    arrived(q_r.at[1], some(1))
    for dh in range(1, 4):
        for d in (2, 1, 3):
            qy_copy(dh, d).start()
    arrived(q_r.at[5], some(5))

    loaded(12)
    loaded(13)

    def rows_of(zz, yy, part):
        halves = []
        for half in range(2):
            g = 2 * part + half
            both = jnp.stack([kq[0, zz, yy, :, g], kq[1, zz, :, yy, g]], axis=1)
            halves.append(both.astype(F32).reshape(16, 128))
        return jnp.concatenate(halves, axis=1)

    decay = dec[head]
    fresh = fre[head]
    fv = fresh * value

    def memory(i, carry):
        at = pl.ds(pl.multiple_of(i * 16, 16), 16)
        zz, yy = head * CUBE + i // 4, i % 4
        q, k = rows_of(zz, yy, 1), rows_of(zz, yy, 0)
        own = norms_v[pl.ds(pl.multiple_of(head * DQK + i * 16, 16), 16)]
        out = []
        for v in range(4):
            new = decay * cells_v[v, at] + fv[v : v + 1] * k
            cells_v[v, at] = new
            prod = q * new
            out.append(carry[v] + prod[0:8] + prod[8:16])
        prod = q * (decay * own + fresh * k)
        out.append(carry[4] + prod[0:8] + prod[8:16])
        return tuple(out)

    sums = lax.fori_loop(0, DQK // 16, memory, (jnp.zeros((8, 256), F32),) * 5)
    denom = jnp.sum(sums[4], axis=0, keepdims=True)
    numer = jnp.concatenate([jnp.sum(sums[v], axis=0, keepdims=True) for v in range(4)], axis=0)
    hidden = numer / jnp.maximum(jnp.abs(denom), 1.0)
    gated = (hidden * outgate).astype(BF16)
    for half in range(2):
        gbuf[half, z, a, core] = gated[:, 128 * half : 128 * (half + 1)]

    for i in range(NZ - 1):
        gz_copy(8 + ((i + 1) // 2) * (2 * (i % 2) - 1)).start()
    arrived(w_r.at[1], rgot.at[pl.ds(0, 7)])
    arrived(q_r.at[2], some(2))
    for dh in range(1, 4):
        for d in (2, 1, 3):
            qx_copy(dh, d).start()
        qd_copy(dh, 0).start()
    arrived(z_r.at[5], gbuf.at[:, pl.ds(0, 15), 0, 0])
    for d in (2, 1, 3):
        ga_copy(d).start()
    arrived(q_r.at[4], some(4))
    for dh in range(1, 4):
        for d in (1, 3, 2):
            qd_copy(dh, d).start()
    arrived(a_r.at[1], gbuf.at[:, :, pl.ds(0, 3), 0])
    w = rgot[...].reshape(64, 512)
    for half in range(2):
        g = gbuf[half].reshape(512, 128)
        mixed = jnp.dot(w, g, preferred_element_type=F32)
        for t in range(4):
            for c in range(NC):
                at = (t * 2 + c) * 8
                rpart[t * 2 + c, :, 128 * half : 128 * (half + 1)] = mixed[at : at + 8]
    start_p(2)
    rgots[core * 4 + r] = rpart[r * 2 + core]

    arrived(q_r.at[6], some(6))

    @pl.loop(0, 64)
    def _(i):
        h = i // 16
        at = pl.ds(pl.multiple_of(i * 16, 16), 16)
        norms_v[at] = dec[h] * norms_v[at] + fre[h] * rows_of(i // 4, i % 4, 0)

    finish_p(2)
    mixed = rgots[0]
    for t in range(1, 8):
        mixed = mixed + rgots[t]
    rows_out[...] = (tok[8, a].astype(F32) + mixed).astype(BF16)

    left(z_s.at[0], tok.at[pl.ds(0, 15), 0])
    left(z_s.at[1], gbuf.at[:, pl.ds(0, 15), 0, 0])
    left(a_s.at[0], tok.at[:, pl.ds(0, 3)])
    left(a_s.at[1], gbuf.at[:, :, pl.ds(0, 3), 0])
    left(w_s.at[0], slices.at[pl.ds(0, 7)])
    left(w_s.at[1], rslices.at[pl.ds(0, 7)])
    for n, ref in enumerate((part, lpart, rpart)):
        left(p_s.at[n], ref.at[pl.ds(0, 7)])
    for n in range(7):
        left(q_s.at[n], some(n))


def put(*refs):
    sems = refs[8]
    copies = [pltpu.make_async_copy(refs[i], refs[4 + i], sems.at[i]) for i in range(4)]
    for copy in copies:
        copy.start()
    for copy in copies:
        copy.wait()


RESULTS = (((8, 256), BF16), ((4, 256, 256), F32), ((1024, 256), F32), ((4, 256), F32))


def step(
    tokens,
    positions,
    norm_gain,
    w_query,
    w_key,
    w_value,
    w_outgate,
    w_input,
    w_forget,
    bias_input,
    bias_forget,
    w_read,
    cells,
    norms,
    maxima,
):
    vmem = pl.BlockSpec(memory_space=pltpu.VMEM)
    hbm = pl.BlockSpec(memory_space=pltpu.HBM)
    dma = pltpu.SemaphoreType.DMA
    operands = (
        tokens,
        positions.reshape(1, 256),
        norm_gain.reshape(32, 128),
        w_query,
        w_key,
        w_value,
        w_outgate,
        w_input,
        w_forget,
        bias_input,
        bias_forget,
        w_read,
        cells,
        norms,
        maxima,
    )
    results = pl.pallas_call(
        kernel,
        out_shape=tuple(pltpu.VMEM(shape, kind) for shape, kind in RESULTS),
        in_specs=[hbm] * 15,
        out_specs=(vmem,) * 4,
        scratch_shapes=[
            pltpu.VMEM((1, 256), jnp.int32),
            pltpu.VMEM((32, 128), F32),
            pltpu.VMEM((2, D), BF16),
            pltpu.VMEM((2, D), BF16),
            pltpu.VMEM((4, D), BF16),
            pltpu.VMEM((4, D), BF16),
            pltpu.VMEM((4, D), BF16),
            pltpu.VMEM((4, D), BF16),
            pltpu.SMEM((4,), F32),
            pltpu.SMEM((4,), F32),
            pltpu.VMEM((8, 2048), BF16),
            pltpu.VMEM((4, 256), F32),
            pltpu.VMEM((NZ, 4, 8, 256), BF16),
            pltpu.VMEM((24, D), F32),
            pltpu.VMEM((8, 16, 1024), BF16),
            pltpu.VMEM((8, 8, 512), BF16),
            pltpu.VMEM((8, 16, 1024), BF16),
            pltpu.VMEM((8, 8, 512), BF16),
            pltpu.VMEM((8, 8, 1024), BF16),
            pltpu.VMEM((NZ, 256, 128), F32),
            pltpu.VMEM((8, 8, 256), F32),
            pltpu.VMEM((8, 8, 256), F32),
            pltpu.VMEM((8, 16, 256), F32),
            pltpu.VMEM((8, 16, 256), F32),
            pltpu.VMEM((8, 8, 256), F32),
            pltpu.VMEM((8, 8, 256), F32),
            pltpu.VMEM((2, NZ, 4, 2, 4, 128), BF16),
            pltpu.VMEM((2, NZ, 4, 4, 4, 2, 128), BF16),
            pltpu.VMEM((4, 1, 256), F32),
            pltpu.VMEM((4, 1, 256), F32),
            dma((8,)),
            dma((2,)),
            dma((6,)),
            dma((2,)),
            dma((2,)),
            dma((2,)),
            dma((2,)),
            dma((3,)),
            dma((3,)),
            dma((7,)),
            dma((7,)),
            dma((4,)),
        ],
        compiler_params=pltpu.CompilerParams(
            collective_id=0, has_side_effects=True, vmem_limit_bytes=40 * 1024 * 1024
        ),
    )(*[pltpu.with_memory_space_constraint(operand, pltpu.HBM) for operand in operands])
    return pl.pallas_call(
        put,
        out_shape=tuple(pltpu.HBM(shape, kind) for shape, kind in RESULTS),
        in_specs=[vmem] * 4,
        out_specs=(hbm,) * 4,
        scratch_shapes=[dma((4,))],
    )(*[pltpu.with_memory_space_constraint(result, pltpu.VMEM) for result in results])


def solution(mesh):
    return jax.shard_map(
        step,
        mesh=mesh,
        in_specs=(
            P("tp", None),
            P(),
            P(),
            P("tp", None),
            P("tp", None),
            P("tp", None),
            P("tp", None),
            P(),
            P(),
            P(),
            P(),
            P("tp", None),
            P("tp", None, None),
            P(),
            P(),
        ),
        out_specs=(P("tp", None), P("tp", None, None), P(), P()),
        check_vma=False,
    )
```

```python
import jax
import jax.numpy as jnp
from jax import lax
from jax.experimental import pallas as pl
from jax.experimental.pallas import tpu as pltpu
from jax.sharding import PartitionSpec as P

DQK = 256
MOST_LEN = 3072
EPS = 1e-06
NZ, NY, NX, NC = 16, 4, 4, 2
CUBE = 4
D = 4096
F32 = jnp.float32
BF16 = jnp.bfloat16
MESH = pl.DeviceIdType.MESH


def kernel(*refs):
    sources, (rows_out, cells_v, norms_v, max_out), rest = refs[:15], refs[15:19], refs[19:]
    held, rest = rest[:12], rest[12:]
    body(sources, held, rows_out, cells_v, norms_v, max_out, *rest)


def body(
    sources,
    held,
    rows_out,
    cells_v,
    norms_v,
    max_out,
    tok,
    rows_v,
    slices,
    rslices,
    wgot,
    rgot,
    wgate,
    gain_b,
    part,
    got,
    lpart,
    lgot,
    rpart,
    rgots,
    gbuf,
    kq,
    dec,
    fre,
    local_sem,
    z_s,
    z_r,
    a_s,
    a_r,
    w_s,
    w_r,
    p_s,
    p_r,
    q_s,
    q_r,
    qz_r,
    qx_r,
):
    me = lax.axis_index("tp")
    core = me % NC
    x = (me // NC) % NX
    y = (me // (NC * NX)) % NY
    z = me // (NC * NX * NY)
    head = z // CUBE
    zlo = z % CUBE
    other = 1 - core
    a = x * other + y * core
    r = y * other + x * core

    def device(zz, yy, xx, cc):
        return (((zz * NY + yy) * NX + xx) * NC + cc,)

    def on_line(cls, t, cc):
        return device(z, t * (1 - cls) + y * cls, x * (1 - cls) + t * cls, cc)

    def send(ref, dst, ss, rs, to):
        return pltpu.make_async_remote_copy(
            src_ref=ref, dst_ref=dst, send_sem=ss, recv_sem=rs, device_id=to, device_id_type=MESH
        )

    (where_ref, gain_ref, wq_ref, wk_ref, wv_ref, wo_ref, wi_ref, wf_ref) = held[:8]
    (bi_ref, bf_ref, wr_ref, maxima_ref) = held[8:]
    targets = (tok.at[8, a],) + held[:11] + (cells_v, norms_v, maxima_ref)
    groups = (0, 2, 1, 1, 1, 1, 1, 1, 1, 3, 4, 1, 5, 6, 7)
    for source, target, group in zip(sources, targets, groups):
        pltpu.make_async_copy(source, target, local_sem.at[group]).start()

    def loaded(i, ref=None):
        target = targets[i] if ref is None else ref
        pltpu.make_async_copy(target, target, local_sem.at[groups[i]]).wait()

    partner = device(z, y, x, other)

    def arrived(sem, ref):
        send(ref, ref, sem, sem, partner).wait_recv()

    def left(sem, ref):
        send(ref, ref, sem, sem, partner).wait_send()

    barrier = pltpu.get_barrier_semaphore()

    def greet(to):
        pl.semaphore_signal(barrier, inc=1, device_id=to, device_id_type=MESH)

    for dz in (3, -3, 2, -2, 1, -1):
        greet(device((z + NZ + dz) % NZ, y, x, core))
    for d in range(1, 4):
        for c in range(NC):
            greet(device(z, (y + d) % NY, x, c))
            greet(device(z, y, (x + d) % NX, c))
    greet(partner)
    pl.semaphore_wait(barrier, 6 + 12 + 1)

    def near_copy(dz):
        to = device((z + NZ + dz) % NZ, y, x, core)
        group = 0 if dz == 3 else 1 if dz == -3 else 2
        return send(tok.at[8, a], tok.at[8 - dz, a], z_s.at[0], z_r.at[group], to)

    def far_copy(dz):
        source, target, group = (5, 5 - dz, 3) if dz > 0 else (11, 11 - dz, 4)
        to = device((z + NZ + dz) % NZ, y, x, core)
        return send(tok.at[source, a], tok.at[target, a], z_s.at[0], z_r.at[group], to)

    def a_copy(n, d):
        mine = tok.at[pl.ds((5, 0, 12)[n], (7, 5, 4)[n]), a]
        to = on_line(other, (a + d) % 4, core)
        return send(mine, mine, a_s.at[0], a_r.at[0], to)

    def gz_copy(dz):
        to = device((z + NZ + dz) % NZ, y, x, core)
        group = 5 if -4 <= dz <= 4 else 6
        return send(
            gbuf.at[:, 8, a, core], gbuf.at[:, 8 - dz, a, core], z_s.at[1], z_r.at[group], to
        )

    def ga_copy(n, d):
        mine = gbuf.at[:, pl.ds((4, 0, 13)[n], (9, 4, 3)[n]), a, core]
        to = on_line(other, (a + d) % 4, core)
        return send(mine, mine, a_s.at[1], a_r.at[1], to)

    loaded(0)
    nearest = (3, -3, 2, -2, 1, -1)
    spread = (8, 7, -7, 6, -6, 5, -5, 4, -4, 3, -3, 2, -2, 1, -1)
    farther = (5, -4, 4, -3, 3, -2, 2, -1, 1)
    for dz in nearest:
        near_copy(dz).start()

    loaded(2, gain_b.at[pl.ds(0, 13), pl.ds(0, 32)])
    rows_v[...] = jnp.concatenate(
        [
            wq_ref[...].astype(F32),
            wk_ref[...].astype(F32),
            jnp.zeros((4, D), F32),
            wv_ref[...].astype(F32),
            wo_ref[...].astype(F32),
            wi_ref[...].astype(F32),
            wf_ref[...].astype(F32),
        ],
        axis=0,
    )
    for p in range(NZ // 2):
        at = slice(128 * p, 128 * (p + 1))
        pair = []
        for s in (2 * p, 2 * p + 1):
            zz = (z + s + 8) % NZ
            pair.append(rows_v[:, pl.ds(pl.multiple_of(zz * 256, 256), 256)])
        for t in range(4):
            by_y = jnp.concatenate([w[:, t * 64 : t * 64 + 64] for w in pair], axis=1)
            by_x = jnp.concatenate(
                [
                    w[:, yy * 64 + t * 16 : yy * 64 + t * 16 + 16]
                    for w in pair
                    for yy in range(4)
                ],
                axis=1,
            )
            for cls, piece in ((0, by_y), (1, by_x)):
                slices[cls * 4 + t, :, at] = piece[0:16].astype(BF16)
                wgate[cls * 4 + t, :, at] = piece[16:24].astype(BF16)
    for p in range(NZ // 4):
        at = slice(128 * p, 128 * (p + 1))
        four = []
        for s in range(4 * p, 4 * p + 4):
            zz = (z + s + 8) % NZ
            four.append(wr_ref[:, pl.ds(pl.multiple_of(zz * 128, 128), 128)].astype(F32))
        for t in range(4):
            rslices[t, :, at] = jnp.concatenate(
                [w[:, t * 32 : t * 32 + 32] for w in four], axis=1
            ).astype(BF16)
            rslices[4 + t, :, at] = jnp.concatenate(
                [w[:, yy * 32 + t * 8 : yy * 32 + t * 8 + 8] for w in four for yy in range(4)],
                axis=1,
            ).astype(BF16)

    gain_t = gain_ref[...].T
    for zz in range(NZ):
        gain_lo = gain_t[:, 2 * zz : 2 * zz + 1]
        gain_hi = gain_t[:, 2 * zz + 1 : 2 * zz + 2]
        gain_b[zz, 0:128] = jnp.broadcast_to(gain_lo, (128, 128))
        gain_b[zz, 128:256] = jnp.broadcast_to(gain_hi, (128, 128))

    def w_copy(cls, d):
        mine = y * (1 - cls) + x * cls
        t = (mine + d) % 4
        to = on_line(cls, t, cls)
        return send(
            slices.at[cls * 4 + t], wgot.at[mine * 2 + core], w_s.at[0], w_r.at[0], to
        )

    def r_copy(cls, d):
        mine = y * (1 - cls) + x * cls
        t = (mine + d) % 4
        to = on_line(cls, t, cls)
        return send(
            rslices.at[cls * 4 + t], rgot.at[mine * 2 + core], w_s.at[1], w_r.at[1], to
        )

    w_copy(other, 0).start()
    for d in (2, 1, 3):
        w_copy(core, d).start()
        w_copy(other, d).start()
    r_copy(other, 0).start()
    for d in (2, 1, 3):
        r_copy(core, d).start()
        r_copy(other, d).start()
    wgot[r * 2 + core] = slices[core * 4 + r]
    rgot[r * 2 + core] = rslices[core * 4 + r]
    for half in range(2):
        gbuf[half, :, :, other] = jnp.zeros((NZ, 4, 4, 128), BF16)

    arrived(z_r.at[0], tok.at[5, a])
    arrived(z_r.at[1], tok.at[11, a])
    for dz in farther:
        far_copy(dz).start()
    arrived(z_r.at[2], tok.at[pl.ds(6, 4), a])
    for d in (2, 1, 3):
        a_copy(0, d).start()
    arrived(z_r.at[3], tok.at[pl.ds(0, 5), a])
    for d in (2, 1, 3):
        a_copy(1, d).start()
    arrived(z_r.at[4], tok.at[pl.ds(12, 4), a])
    for d in (2, 1, 3):
        a_copy(2, d).start()

    arrived(w_r.at[0], wgot.at[pl.ds(0, 7)])
    arrived(a_r.at[0], tok.at[:, pl.ds(0, 3)])

    acc = jnp.zeros((128, 256), F32)
    gates = jnp.zeros((8, 256), F32)
    squares = jnp.zeros((8, 256), F32)
    first = core == 0
    for p in range(4):
        blocks = []
        for zz in range(4 * p, 4 * p + 4):
            for aa in range(4):
                t = tok[zz, aa].astype(F32)
                squares = squares + t * t
                row = (y * other + aa * core) * 64 + (aa * other + x * core) * 16 + core * 8
                g = gain_b[(z + zz + 8) % NZ, pl.ds(pl.multiple_of(row, 8), 8)]
                t = t * jnp.concatenate([g, g], axis=1)
                none = jnp.zeros_like(t)
                blocks.append(jnp.where(first, t, none))
                blocks.append(jnp.where(first, none, t))
        normed = jnp.concatenate(blocks, axis=0).astype(BF16)
        at = slice(256 * p, 256 * (p + 1))
        w = wgot[:, :, at].reshape(128, 256)
        acc = acc + jnp.dot(w, normed, preferred_element_type=F32)
        gates = gates + jnp.dot(wgate[core * 4 + r, :, at], normed, preferred_element_type=F32)
    total = jnp.sum(squares, axis=0, keepdims=True)
    for t in range(4):
        for c in range(NC):
            at = (t * 2 + c) * 16
            part[t * 2 + c, 0:4] = acc[at : at + 4]
            part[t * 2 + c, 4:5] = total

    def p_copy(n, c, d):
        t = (r + d) % 4
        source, target = ((part, got), (lpart, lgot), (rpart, rgots))[n]
        to = on_line(core, t, c)
        return send(source.at[t * 2 + c], target.at[core * 4 + r], p_s.at[n], p_r.at[n], to)

    def start_p(n):
        for d in (2, 1, 3):
            p_copy(n, core, d).start()
            p_copy(n, other, d).start()
        p_copy(n, other, 0).start()

    def finish_p(n):
        arrived(p_r.at[n], (got, lgot, rgots)[n].at[pl.ds(0, 7)])

    start_p(0)
    for t in range(4):
        for c in range(NC):
            at = (t * 2 + c) * 16
            lpart[t * 2 + c, 0:8] = acc[at + 8 : at + 16]
            lpart[t * 2 + c, 8:16] = gates
    start_p(1)
    got[core * 4 + r] = part[r * 2 + core]
    lgot[core * 4 + r] = lpart[r * 2 + core]
    for i in (1, 9, 10, 14):
        loaded(i)
    length = 1.0 + where_ref[...].astype(F32) / MOST_LEN
    finish_p(0)
    sums = got[0]
    for t in range(1, 8):
        sums = sums + got[t]
    scale = lax.rsqrt(sums[4:5] / D + EPS)
    proj = sums[0:4] * scale
    query = proj[0:2].astype(BF16)
    key = (proj[2:4] * DQK ** (-0.5)).astype(BF16)
    for half in range(2):
        kq[core, z, r, a, half] = key[:, 128 * half : 128 * (half + 1)]
        kq[core, z, r, a, 2 + half] = query[:, 128 * half : 128 * (half + 1)]

    def place(zz, tr, ta):
        return device(zz, tr * other + ta * core, ta * other + tr * core, core)

    def zs_of(dh):
        return pl.ds(((head + 4 - dh) % 4) * CUBE, CUBE)

    def parts(dh):
        return pl.ds(0, 4 if dh == 0 else 2)

    def qz_copy(dz, dr):
        mine = kq.at[core, z, r, a]
        to = place(head * CUBE + (zlo + dz) % CUBE, (r + dr) % 4, a)
        return send(mine, mine, q_s.at[0], qz_r.at[dz], to)

    def kz_copy(dh, j):
        mine = kq.at[core, z, r, a, pl.ds(0, 2)]
        to = place(((head + dh) % 4) * CUBE + (zlo + j) % CUBE, r, a)
        return send(mine, mine, q_s.at[1], q_r.at[1], to)

    def qy_copy(dh, d):
        mine = kq.at[core, zs_of(dh), r, a, parts(dh)]
        return send(mine, mine, q_s.at[2], q_r.at[2], place(z, (r + d) % 4, a))

    def q_plane(dz, d):
        mine = kq.at[core, head * CUBE + (zlo + CUBE - dz) % CUBE, :, a]
        return send(mine, mine, q_s.at[3], qx_r.at[d], place(z, r, (a + d) % 4))

    def qx_copy(dh, d):
        mine = kq.at[core, zs_of(dh), :, a, parts(dh)]
        return send(mine, mine, q_s.at[4], q_r.at[4], place(z, r, (a + d) % 4))

    def qd_copy(dh, d):
        this = kq.at[core, zs_of(dh), :, (a + 4 - d) % 4, parts(dh)]
        n = 5 if dh == 0 else 6
        return send(this, this, q_s.at[n], q_r.at[n], partner)

    def some(n):
        return (
            kq.at[0, pl.ds(0, 15), 0, 0],
            kq.at[0, pl.ds(0, 12), 0, 0, pl.ds(0, 2)],
            kq.at[0, pl.ds(0, 9), :, 0, pl.ds(0, 2)],
            kq.at[0, pl.ds(0, 12), :, 0],
            kq.at[0, pl.ds(0, 9), :, :, pl.ds(0, 2)],
            kq.at[0, :, :, 0],
            kq.at[0, pl.ds(0, 12), :, :, pl.ds(0, 2)],
        )[n]

    near = [(dz, dy) for dz in range(4) for dy in range(4) if dz or dy]
    for dz, dy in sorted(near, key=lambda at: (-(at[0] > 1) - (at[1] == 2), at)):
        qz_copy(dz, dy).start()
    for dh in (2, 1, 3):
        for j in range(CUBE):
            kz_copy(dh, j).start()

    finish_p(1)
    sums = lgot[0]
    for t in range(1, 8):
        sums = sums + lgot[t]
    proj = sums * scale
    value = proj[0:4]
    outgate = jax.nn.sigmoid(proj[4:8])
    for h in range(4):
        gate_in = proj[8 + h : 9 + h] + bi_ref[h]
        forget = proj[12 + h : 13 + h] + bf_ref[h]
        logf = (jnp.minimum(forget, 0.0) - jnp.log1p(jnp.exp(-jnp.abs(forget)))) * length
        held_max = logf + maxima_ref[h : h + 1]
        new_max = jnp.maximum(held_max, gate_in)
        max_out[h : h + 1] = new_max
        dec[h] = jnp.exp(held_max - new_max)
        fre[h] = jnp.exp(gate_in - new_max)

    for dz in (0, 1, 3, 2):
        arrived(qz_r.at[dz], kq.at[0, pl.ds(0, 3 if dz == 0 else 4), 0, 0])
        for d in (2, 1, 3):
            q_plane(dz, d).start()
    qd_copy(0, 0).start()
    for d in (1, 3, 2):
        arrived(qx_r.at[d], kq.at[0, pl.ds(0, 4), :, 0])
        qd_copy(0, d).start()
    arrived(q_r.at[1], some(1))
    for dh in range(1, 4):
        for d in (2, 1, 3):
            qy_copy(dh, d).start()
    arrived(q_r.at[5], some(5))

    loaded(12)
    loaded(13)

    def rows_of(zz, yy, part):
        halves = []
        for half in range(2):
            g = 2 * part + half
            both = jnp.stack([kq[0, zz, yy, :, g], kq[1, zz, :, yy, g]], axis=1)
            halves.append(both.astype(F32).reshape(16, 128))
        return jnp.concatenate(halves, axis=1)

    decay = dec[head]
    fresh = fre[head]
    fv = fresh * value

    def memory(i, carry):
        at = pl.ds(pl.multiple_of(i * 16, 16), 16)
        zz, yy = head * CUBE + i // 4, i % 4
        q, k = rows_of(zz, yy, 1), rows_of(zz, yy, 0)
        own = norms_v[pl.ds(pl.multiple_of(head * DQK + i * 16, 16), 16)]
        out = []
        for v in range(4):
            new = decay * cells_v[v, at] + fv[v : v + 1] * k
            cells_v[v, at] = new
            prod = q * new
            out.append(carry[v] + prod[0:8] + prod[8:16])
        prod = q * (decay * own + fresh * k)
        out.append(carry[4] + prod[0:8] + prod[8:16])
        return tuple(out)

    sums = lax.fori_loop(0, DQK // 16, memory, (jnp.zeros((8, 256), F32),) * 5)
    denom = jnp.sum(sums[4], axis=0, keepdims=True)
    numer = jnp.concatenate([jnp.sum(sums[v], axis=0, keepdims=True) for v in range(4)], axis=0)
    hidden = numer / jnp.maximum(jnp.abs(denom), 1.0)
    gated = (hidden * outgate).astype(BF16)
    for half in range(2):
        gbuf[half, 8, a, core] = gated[:, 128 * half : 128 * (half + 1)]

    for dz in spread:
        gz_copy(dz).start()
    arrived(w_r.at[1], rgot.at[pl.ds(0, 7)])
    arrived(q_r.at[2], some(2))
    for dh in range(1, 4):
        for d in (2, 1, 3):
            qx_copy(dh, d).start()
        qd_copy(dh, 0).start()
    arrived(z_r.at[5], gbuf.at[:, pl.ds(0, 8), 0, 0])
    for d in (2, 1, 3):
        ga_copy(0, d).start()
    arrived(z_r.at[6], gbuf.at[:, pl.ds(0, 7), 0, 0])
    for n in (1, 2):
        for d in (2, 1, 3):
            ga_copy(n, d).start()
    arrived(q_r.at[4], some(4))
    for dh in range(1, 4):
        for d in (1, 3, 2):
            qd_copy(dh, d).start()
    arrived(a_r.at[1], gbuf.at[:, :, pl.ds(0, 3), 0])
    w = rgot[...].reshape(64, 512)
    for half in range(2):
        g = gbuf[half].reshape(512, 128)
        mixed = jnp.dot(w, g, preferred_element_type=F32)
        for t in range(4):
            for c in range(NC):
                at = (t * 2 + c) * 8
                rpart[t * 2 + c, :, 128 * half : 128 * (half + 1)] = mixed[at : at + 8]
    start_p(2)
    rgots[core * 4 + r] = rpart[r * 2 + core]

    arrived(q_r.at[6], some(6))

    @pl.loop(0, 64)
    def _(i):
        h = i // 16
        at = pl.ds(pl.multiple_of(i * 16, 16), 16)
        norms_v[at] = dec[h] * norms_v[at] + fre[h] * rows_of(i // 4, i % 4, 0)

    finish_p(2)
    mixed = rgots[0]
    for t in range(1, 8):
        mixed = mixed + rgots[t]
    rows_out[...] = (tok[8, a].astype(F32) + mixed).astype(BF16)

    left(z_s.at[0], tok.at[pl.ds(0, 15), 0])
    left(z_s.at[1], gbuf.at[:, pl.ds(0, 15), 0, 0])
    left(a_s.at[0], tok.at[:, pl.ds(0, 3)])
    left(a_s.at[1], gbuf.at[:, :, pl.ds(0, 3), 0])
    left(w_s.at[0], slices.at[pl.ds(0, 7)])
    left(w_s.at[1], rslices.at[pl.ds(0, 7)])
    for n, ref in enumerate((part, lpart, rpart)):
        left(p_s.at[n], ref.at[pl.ds(0, 7)])
    for n in range(7):
        left(q_s.at[n], some(n))


def put(*refs):
    sems = refs[8]
    copies = [pltpu.make_async_copy(refs[i], refs[4 + i], sems.at[i]) for i in range(4)]
    for copy in copies:
        copy.start()
    for copy in copies:
        copy.wait()


RESULTS = (((8, 256), BF16), ((4, 256, 256), F32), ((1024, 256), F32), ((4, 256), F32))


def step(
    tokens,
    positions,
    norm_gain,
    w_query,
    w_key,
    w_value,
    w_outgate,
    w_input,
    w_forget,
    bias_input,
    bias_forget,
    w_read,
    cells,
    norms,
    maxima,
):
    vmem = pl.BlockSpec(memory_space=pltpu.VMEM)
    hbm = pl.BlockSpec(memory_space=pltpu.HBM)
    dma = pltpu.SemaphoreType.DMA
    operands = (
        tokens,
        positions.reshape(1, 256),
        norm_gain.reshape(32, 128),
        w_query,
        w_key,
        w_value,
        w_outgate,
        w_input,
        w_forget,
        bias_input,
        bias_forget,
        w_read,
        cells,
        norms,
        maxima,
    )
    results = pl.pallas_call(
        kernel,
        out_shape=tuple(pltpu.VMEM(shape, kind) for shape, kind in RESULTS),
        in_specs=[hbm] * 15,
        out_specs=(vmem,) * 4,
        scratch_shapes=[
            pltpu.VMEM((1, 256), jnp.int32),
            pltpu.VMEM((32, 128), F32),
            pltpu.VMEM((2, D), BF16),
            pltpu.VMEM((2, D), BF16),
            pltpu.VMEM((4, D), BF16),
            pltpu.VMEM((4, D), BF16),
            pltpu.VMEM((4, D), BF16),
            pltpu.VMEM((4, D), BF16),
            pltpu.SMEM((4,), F32),
            pltpu.SMEM((4,), F32),
            pltpu.VMEM((8, 2048), BF16),
            pltpu.VMEM((4, 256), F32),
            pltpu.VMEM((NZ, 4, 8, 256), BF16),
            pltpu.VMEM((24, D), F32),
            pltpu.VMEM((8, 16, 1024), BF16),
            pltpu.VMEM((8, 8, 512), BF16),
            pltpu.VMEM((8, 16, 1024), BF16),
            pltpu.VMEM((8, 8, 512), BF16),
            pltpu.VMEM((8, 8, 1024), BF16),
            pltpu.VMEM((NZ, 256, 128), F32),
            pltpu.VMEM((8, 8, 256), F32),
            pltpu.VMEM((8, 8, 256), F32),
            pltpu.VMEM((8, 16, 256), F32),
            pltpu.VMEM((8, 16, 256), F32),
            pltpu.VMEM((8, 8, 256), F32),
            pltpu.VMEM((8, 8, 256), F32),
            pltpu.VMEM((2, NZ, 4, 2, 4, 128), BF16),
            pltpu.VMEM((2, NZ, 4, 4, 4, 2, 128), BF16),
            pltpu.VMEM((4, 1, 256), F32),
            pltpu.VMEM((4, 1, 256), F32),
            dma((8,)),
            dma((2,)),
            dma((7,)),
            dma((2,)),
            dma((2,)),
            dma((2,)),
            dma((2,)),
            dma((3,)),
            dma((3,)),
            dma((7,)),
            dma((7,)),
            dma((4,)),
            dma((4,)),
        ],
        compiler_params=pltpu.CompilerParams(
            collective_id=0, has_side_effects=True, vmem_limit_bytes=40 * 1024 * 1024
        ),
    )(*[pltpu.with_memory_space_constraint(operand, pltpu.HBM) for operand in operands])
    return pl.pallas_call(
        put,
        out_shape=tuple(pltpu.HBM(shape, kind) for shape, kind in RESULTS),
        in_specs=[vmem] * 4,
        out_specs=(hbm,) * 4,
        scratch_shapes=[dma((4,))],
    )(*[pltpu.with_memory_space_constraint(result, pltpu.VMEM) for result in results])


def solution(mesh):
    return jax.shard_map(
        step,
        mesh=mesh,
        in_specs=(
            P("tp", None),
            P(),
            P(),
            P("tp", None),
            P("tp", None),
            P("tp", None),
            P("tp", None),
            P(),
            P(),
            P(),
            P(),
            P("tp", None),
            P("tp", None, None),
            P(),
            P(),
        ),
        out_specs=(P("tp", None), P("tp", None, None), P(), P()),
        check_vma=False,
    )
```
